256 devices in a mesh: ep: 64 (over z, y, core), tp: 4 (over x).
Axes of the slice: x: 4, y: 4, z: 8, core: 2. Of those that a mesh axis runs over, the one named last changes fastest.
Arguments:
- tokens: bfloat16 [512, 2048], P('ep'), may hold values from -4 to 4
- w_query: bfloat16 [2048, 1024], P(None, 'tp'), may hold values from -0.125 to 0.125
- w_key: bfloat16 [2048, 1024], P(None, 'tp'), may hold values from -0.125 to 0.125
- w_value: bfloat16 [2048, 1024], P(None, 'tp'), may hold values from -0.125 to 0.125
- w_outgate: bfloat16 [2048, 1024], P(None, 'tp'), may hold values from -0.125 to 0.125
- w_igate: bfloat16 [2048, 4], P(None, 'tp'), may hold values from -0.125 to 0.125
- w_fgate: bfloat16 [2048, 4], P(None, 'tp'), may hold values from -0.125 to 0.125
- forget_bias: float32 [4], P('tp'), may hold values from -1 to 5
- w_out: bfloat16 [1024, 2048], P('tp'), may hold values from -0.1875 to 0.1875
- gain_mix: float32 [2048], replicated, may hold values from 0.1 to 1.9
- gain_moe: float32 [2048], replicated, may hold values from 0.1 to 1.9
- memory: float32 [512, 4, 256, 256], P('ep', 'tp'), may hold values from -0.4 to 0.4
- normalizer: float32 [512, 4, 256], P('ep', 'tp'), may hold values from -0.8 to 0.8
- stabilizer: float32 [512, 4], P('ep', 'tp'), may hold values from 0 to 2
- expert_gate: bfloat16 [64, 2048, 512], P('ep', None, 'tp'), may hold values from -0.125 to 0.125
- expert_up: bfloat16 [64, 2048, 512], P('ep', None, 'tp'), may hold values from -0.125 to 0.125
- expert_down: bfloat16 [64, 512, 2048], P('ep', 'tp'), may hold values from -1 to 1
- routes: int32 [512, 4], P('ep'), may hold values from 0 to 63, all different within a row; in each aligned block of 8 rows (0 to 7, 8 to 15, ...) at most 2 rows name the same one
- route_weight: float32 [512, 4], P('ep'), may hold values from 0.2 to 1
Outputs:
- output: bfloat16 [512, 2048], P('ep', 'tp')
- memory_next: float32 [512, 4, 256, 256], P('ep', 'tp')
- norm_next: float32 [512, 4, 256], P('ep', 'tp')
- stabilizer_next: float32 [512, 4], P('ep', 'tp')
The draws below stay inside these ranges and needn't reach their ends.
Inputs may be any that keep to these rules, and one draw needn't show every extreme that they name: `routes`: each row names 4 different experts. Among the 8 rows of one device (aligned blocks), no expert is named more than 2 times, a bound that some block reaches.
All inputs are finite; a program needn't handle non-finite values.
Results may differ from the reference program's by a relative error of at most 0.029.
Values may be sent and summed in bfloat16 or wider, within the bound.
A program may use at most 64 MiB of HBM per device.

```python
import math
import jax
import jax.numpy as jnp
import numpy as np
from jax import lax

D = 2048
NH = 4
DH = 256
FF = 512
TOP = 4
SEQ_DEV = 8
TOKENS = 512
EXPERTS = 64
CAP = 2
N_EP = 64


def steps_of(stream_key, shape, pieces, least, high):
    loudness = 1.0
    for position, parts in pieces:
        steps = jax.random.uniform(jax.random.fold_in(jax.random.fold_in(stream_key, 6), position), (parts,), jnp.float32, least / len(pieces), high / len(pieces))
        loudness = loudness * jnp.repeat(jnp.exp(steps), shape[position] // parts).reshape((-1,) + (1,) * (len(shape) - 1 - position))
    return loudness


def routed_block(rng, own, number, rows, count, top, reach, slope):
    order = jax.random.permutation(rng, count)
    crowded, ordinary = load_shares(count, rows * top, reach, slope, True), load_shares(count, rows * top, reach, slope, False)
    places = jnp.arange(count)

    def named(tallies, offset_by):
        used = int((tallies > 0).sum())
        fixed = max(1, used // 4)
        passed = fixed + (places - fixed + offset_by * (used - fixed)) % max(1, count - fixed)
        return jnp.zeros((count,), jnp.int32).at[order[jnp.where(places < fixed, places, passed)]].set(jnp.asarray(tallies, jnp.int32))

    tallies = jnp.where(number % 4 == 0, named(crowded, number // 4), named(ordinary, number - number // 4 - 1))
    mixed = jax.random.permutation(jax.random.fold_in(own, 3), count)
    giver, sink = mixed[0:count // 2 * 2:2], mixed[1:count // 2 * 2:2]
    margin = jnp.minimum(tallies[giver] - 1, reach - tallies[sink]) // 2
    margin = jnp.where((giver == order[0]) | (sink == order[0]) | (tallies[sink] == 0), 0, jnp.maximum(margin, 0))
    passed = jax.random.randint(jax.random.fold_in(own, 4), (count // 2,), 0, 1 << 20) % (margin + 1)
    tallies = tallies.at[giver].add(-passed).at[sink].add(passed)
    items = jnp.searchsorted(jnp.cumsum(tallies), jnp.arange(rows * top), side="right").astype(jnp.int32)
    grid = items.reshape(top, rows).T
    grid = grid[jax.random.permutation(jax.random.fold_in(own, 1), rows)]
    offset_by = jax.random.randint(jax.random.fold_in(own, 2), (rows, 1), 0, top)
    return jnp.take_along_axis(grid, (jnp.arange(top)[None, :] + offset_by) % top, axis=1)


def load_shares(count, total, reach, slope, full):
    loads = [(1 << 20) // math.isqrt(standing ** slope) + 1 for standing in range(1, count + 1)]
    largest = reach if full else min(reach, max(-(-total // count), total * loads[0] // sum(loads)))
    least = 1 if total - largest >= count - 1 else 0
    counts, spare = [largest] + [least] * (count - 1), total - largest - least * (count - 1)
    while spare > 0:
        free = [i for i in range(1, count) if counts[i] < largest] or [i for i in range(1, count) if counts[i] < reach]
        mass, left = sum([loads[i] for i in free]), spare
        for i in free:
            more = min(reach - counts[i], max(1, left * loads[i] // mass), spare)
            counts[i] = counts[i] + more
            spare = spare - more
    return np.array(counts)


def scatter_about(stream_key, extent, deviation, reach, split=(), held_as=jnp.bfloat16):
    values = jax.random.normal(stream_key, extent, jnp.float32) * deviation
    if len(split) > 0:
        values = steps_of(stream_key, extent, split, -0.22, 0.18) * values
    return jnp.clip(values, min=-reach, max=reach).astype(held_as)


def setup_inputs(seed: int = 0) -> dict:
    key_list = jax.random.split(jax.random.key(seed), 20)
    tokens = scatter_about(key_list[0], (TOKENS, D), 1.0, 4.0, ((0, 64),))
    w_query = scatter_about(key_list[1], (D, NH * DH), D ** -0.5, 0.125, ((1, 4),))
    w_key = scatter_about(key_list[2], (D, NH * DH), D ** -0.5, 0.125, ((1, 4),))
    w_value = scatter_about(key_list[3], (D, NH * DH), D ** -0.5, 0.125, ((1, 4),))
    w_outgate = scatter_about(key_list[4], (D, NH * DH), D ** -0.5, 0.125, ((1, 4),))
    w_igate = scatter_about(key_list[5], (D, NH), D ** -0.5, 0.125, ((1, 4),))
    w_fgate = scatter_about(key_list[6], (D, NH), D ** -0.5, 0.125, ((1, 4),))
    forget_bias = jnp.clip(-1.0 + 6.0 * jax.random.uniform(key_list[7], (NH,), jnp.float32) ** steps_of(key_list[7], (NH,), ((0, 4),), -0.2, 0.2), -1.0, 5.0)
    w_out = scatter_about(key_list[8], (NH * DH, D), (NH * DH) ** -0.5, 0.1875, ((0, 4),))
    gain_mix = jnp.clip(1.0 + 0.18 * jax.random.normal(key_list[9], (D,), jnp.float32), 0.1, 1.9)
    gain_moe = jnp.clip(1.0 + 0.18 * jax.random.normal(key_list[10], (D,), jnp.float32), 0.1, 1.9)
    memory = scatter_about(key_list[11], (TOKENS, NH, DH, DH), 0.05, 0.4, ((0, 64), (1, 4)), jnp.float32)
    normalizer = scatter_about(key_list[12], (TOKENS, NH, DH), 0.1, 0.8, ((0, 64), (1, 4)), jnp.float32)
    stabilizer = jnp.clip(2.0 * jax.random.uniform(key_list[13], (TOKENS, NH), jnp.float32) ** steps_of(key_list[13], (TOKENS, NH), ((0, 64), (1, 4)), -0.2, 0.2), 0.0, 2.0)
    expert_gate = scatter_about(key_list[14], (EXPERTS, D, FF), D ** -0.5, 0.125, ((0, 64), (2, 4)))
    expert_up = scatter_about(key_list[15], (EXPERTS, D, FF), D ** -0.5, 0.125, ((0, 64), (2, 4)))
    expert_down = scatter_about(key_list[16], (EXPERTS, FF, D), (FF // 16) ** -0.5, 1.0, ((0, 64), (1, 4)))
    routes_keys = jax.random.split(jax.random.fold_in(key_list[17], 1), TOKENS // SEQ_DEV)
    routes_turns = jax.random.permutation(jax.random.fold_in(key_list[17], 3), TOKENS // SEQ_DEV)
    routes = jax.vmap(lambda own, number: routed_block(jax.random.fold_in(key_list[17], 2), own, number, SEQ_DEV, EXPERTS, TOP, CAP, 2))(routes_keys, routes_turns).reshape((TOKENS, TOP))
    route_weight = jnp.clip(0.2 + 0.8 * jax.random.uniform(key_list[18], (TOKENS, TOP), jnp.float32) ** steps_of(key_list[18], (TOKENS, TOP), ((0, 64),), -0.2, 0.2), 0.2, 1.0)
    return dict(tokens=tokens, w_query=w_query, w_key=w_key, w_value=w_value, w_outgate=w_outgate, w_igate=w_igate, w_fgate=w_fgate, forget_bias=forget_bias, w_out=w_out, gain_mix=gain_mix, gain_moe=gain_moe, memory=memory, normalizer=normalizer, stabilizer=stabilizer, expert_gate=expert_gate, expert_up=expert_up, expert_down=expert_down, routes=routes, route_weight=route_weight)


def layer_norm(row_data, gain_vec):
    values = row_data.astype(jnp.float32)
    row_mean = lax.optimization_barrier(jnp.mean(values, -1, keepdims=True))
    centered = values - row_mean
    variance = lax.optimization_barrier(jnp.mean(centered * centered, -1, keepdims=True))
    return centered * lax.rsqrt(variance + 1e-05) * gain_vec

def slot_targets(routes, experts, capacity):
    flat_routes = routes.reshape(-1)
    onehot = (flat_routes[:, None] == jnp.arange(experts, dtype=jnp.int32)[None, :]).astype(jnp.int32)
    before = jnp.cumsum(onehot, axis=0) - onehot
    slot_index = lax.optimization_barrier(jnp.sum(before * onehot, axis=1))
    return (flat_routes * capacity + slot_index).astype(jnp.int32)

def expert_rows(operands):
    rows_in, gate_weight, up_weight, down_weight = operands
    gate_part = jnp.dot(rows_in, gate_weight, preferred_element_type=jnp.float32)
    up_part = jnp.dot(rows_in, up_weight, preferred_element_type=jnp.float32)
    hidden = (jax.nn.silu(gate_part) * up_part).astype(jnp.bfloat16)
    return jnp.dot(hidden, down_weight, preferred_element_type=jnp.float32).astype(jnp.bfloat16)

def reference(tokens, w_query, w_key, w_value, w_outgate, w_igate, w_fgate, forget_bias, w_out, gain_mix, gain_moe, memory, normalizer, stabilizer, expert_gate, expert_up, expert_down, routes, route_weight):
    normed = layer_norm(tokens, gain_mix).astype(jnp.bfloat16)

    def project(weight):
        rounded = jnp.dot(normed, weight, preferred_element_type=jnp.float32).astype(jnp.bfloat16)
        rounded = lax.optimization_barrier(rounded)
        return rounded.astype(jnp.float32).reshape(TOKENS, NH, DH)
    queries = project(w_query)
    keys_scaled = project(w_key) / math.sqrt(DH)
    values_rows = project(w_value)
    out_gate = project(w_outgate)
    gate_in = jnp.dot(normed, w_igate, preferred_element_type=jnp.float32)
    gate_forget = jnp.dot(normed, w_fgate, preferred_element_type=jnp.float32)
    log_forget = jax.nn.log_sigmoid(gate_forget + forget_bias)
    stabilizer_next = jnp.maximum(log_forget + stabilizer, gate_in)
    keep_rate = jnp.exp(log_forget + stabilizer - stabilizer_next)
    admit_rate = jnp.exp(gate_in - stabilizer_next)
    memory_next = keep_rate[:, :, None, None] * memory + admit_rate[:, :, None, None] * keys_scaled[:, :, :, None] * values_rows[:, :, None, :]
    norm_next = keep_rate[:, :, None] * normalizer + admit_rate[:, :, None] * keys_scaled
    numerator = jnp.einsum('thk,thkv->thv', queries, memory_next, precision=lax.Precision.HIGHEST)
    denominator = lax.optimization_barrier(jnp.sum(queries * norm_next, axis=-1))
    readout = numerator / jnp.maximum(jnp.abs(denominator), jnp.exp(-stabilizer_next))[:, :, None]
    mixed = (jax.nn.sigmoid(out_gate) * readout).astype(jnp.bfloat16)
    head_part = jnp.einsum('thd,hde->the', mixed.astype(jnp.float32), w_out.reshape(NH, DH, D).astype(jnp.float32)).astype(jnp.bfloat16)
    residual = tokens.astype(jnp.float32) + lax.optimization_barrier(jnp.sum(head_part.astype(jnp.float32), axis=1))
    expert_in = layer_norm(residual, gain_moe).astype(jnp.bfloat16)
    blocks = routes.reshape(N_EP, SEQ_DEV * TOP)
    local_target = jax.vmap(lambda route_row: slot_targets(route_row, EXPERTS, CAP))(blocks)
    slot_index = local_target - blocks * CAP
    block_index = jnp.arange(N_EP, dtype=jnp.int32)[:, None]
    placement = ((blocks * N_EP + block_index) * CAP + slot_index).reshape(-1).astype(jnp.int32)
    buffer = jnp.zeros((EXPERTS * N_EP * CAP, D), jnp.bfloat16).at[placement].set(jnp.repeat(expert_in, TOP, axis=0))
    expert_outs = lax.map(expert_rows, (buffer.reshape(EXPERTS, N_EP * CAP, D), expert_gate, expert_up, expert_down))
    picked = expert_outs.reshape(-1, D)[placement].reshape(TOKENS, TOP, D)
    combined = lax.optimization_barrier(jnp.sum(route_weight[:, :, None] * picked.astype(jnp.float32), axis=1))
    output = (residual + combined).astype(jnp.bfloat16)
    return (output, memory_next, norm_next, stabilizer_next)
```

```python
import functools

import jax
import jax.numpy as jnp
from jax import lax
from jax.experimental import pallas as pl
from jax.experimental.pallas import tpu as pltpu
from jax.sharding import PartitionSpec as P

F32 = jnp.float32
BF16 = jnp.bfloat16
MESH = pl.DeviceIdType.MESH

ROWS = 8
WIDTH = 2048
HEAD = 256
HIDDEN = 128
TOP = 4
NEP = 64
NTP = 4
CAP = 2
SLOTS = NEP * CAP
LANES = 128
CHUNKS = WIDTH // LANES
QUARTER = WIDTH // NTP
QCHUNKS = QUARTER // LANES
MSG = CHUNKS * CAP
QMSG = QCHUNKS * CAP
PITCH = 40
BIG = 1 << 20


def layer_norm(values, gain):
    mean = jnp.mean(values, -1, keepdims=True)
    centered = values - mean
    variance = jnp.mean(centered * centered, -1, keepdims=True)
    return centered * lax.rsqrt(variance + 1e-05) * gain


def iota(shape, dim):
    return lax.broadcasted_iota(jnp.int32, shape, dim)


def column(row, size):
    eye = iota((size, size), 0) == iota((size, size), 1)
    return jnp.sum(jnp.where(eye, row, 0.0), axis=1, keepdims=True)


def partner(me, k):
    a, b = k // 8, k % 8
    dz = 4 + (a // 2) * (1 - 2 * (a % 2)) - (a % 2)
    m = b // 2
    dy = 2 + (m // 2) * (1 - 2 * (m % 2)) - (m % 2)
    dc = 1 - b % 2
    z, y, c = me // 8, (me // 2) % 4, me % 2
    return (((z + dz) % 8) * 4 + (y + dy) % 4) * 2 + (c + dc) % 2


def kernel(
    tokens,
    gain_mix,
    gain_moe,
    w_igate,
    w_fgate,
    forget_bias,
    normalizer,
    stabilizer,
    routes,
    route_weight,
    w_key,
    w_value,
    w_query,
    w_outgate,
    memory,
    w_out,
    expert_gate,
    expert_up,
    expert_down,
    output,
    memory_next,
    norm_next,
    stabilizer_next,
    w_buf,
    mem_buf,
    out_buf,
    gu_buf,
    down_buf,
    num_buf,
    res_buf,
    heads,
    pick_buf,
    stage,
    disp_send,
    disp_recv,
    part_send,
    part_recv,
    ret_stage,
    ret_send,
    ret_recv,
    load_sem,
    store_sem,
    head_sems,
    disp_sems,
    part_sems,
    ret_sems,
):
    ep = lax.axis_index("ep")
    tp = lax.axis_index("tp")

    barrier = pltpu.get_barrier_semaphore()

    def greet(k, carry):
        pl.semaphore_signal(
            barrier, inc=1, device_id=(partner(ep, k), tp), device_id_type=MESH
        )
        return carry

    loads = [
        pltpu.make_async_copy(w, w_buf.at[i], load_sem.at[i])
        for i, w in enumerate((w_key, w_value, w_query, w_outgate))
    ]
    loads.append(pltpu.make_async_copy(memory.at[:, 0], mem_buf, load_sem.at[4]))
    loads.append(pltpu.make_async_copy(w_out, out_buf, load_sem.at[5]))
    loads.append(
        pltpu.make_async_copy(expert_gate.at[0], gu_buf.at[:, pl.ds(0, HIDDEN)], load_sem.at[6])
    )
    loads.append(
        pltpu.make_async_copy(
            expert_up.at[0], gu_buf.at[:, pl.ds(HIDDEN, HIDDEN)], load_sem.at[7]
        )
    )
    for q in range(NTP):
        loads.append(
            pltpu.make_async_copy(
                expert_down.at[0, :, pl.ds(q * QUARTER, QUARTER)],
                down_buf.at[q],
                load_sem.at[8 + q],
            )
        )
    for load in loads:
        load.start()

    lax.fori_loop(0, NEP - 1, greet, 0)
    for d in range(1, NTP):
        pl.semaphore_signal(
            barrier, inc=1, device_id=(ep, (tp + d) % NTP), device_id_type=MESH
        )

    token_rows = tokens[...].astype(F32)
    normed = layer_norm(token_rows, gain_mix[...]).astype(BF16)
    wide = normed.astype(F32)
    gate_in = jnp.sum(wide * w_igate[...].astype(F32), axis=1, keepdims=True)
    gate_forget = jnp.sum(wide * w_fgate[...].astype(F32), axis=1, keepdims=True)
    shifted = gate_forget + forget_bias[0]
    log_forget = jnp.minimum(shifted, 0.0) - jnp.log1p(jnp.exp(-jnp.abs(shifted)))
    carried = log_forget + column(stabilizer[...], ROWS)
    stab = jnp.maximum(carried, gate_in)
    keep = jnp.exp(carried - stab)
    admit = jnp.exp(gate_in - stab)
    eye = iota((ROWS, ROWS), 0) == iota((ROWS, ROWS), 1)
    stabilizer_next[...] = jnp.sum(jnp.where(eye, stab, 0.0), axis=0, keepdims=True)

    def project(i):
        loads[i].wait()
        product = jnp.dot(normed, w_buf[i], preferred_element_type=F32)
        return product.astype(BF16).astype(F32)

    keys = project(0) * (1.0 / 16.0)
    values = project(1)
    queries = project(2)
    admitted = admit * keys
    new_norm = keep * normalizer[:, 0, :] + admitted
    norm_next[:, 0, :] = new_norm
    denominator = jnp.sum(queries * new_norm, axis=1, keepdims=True)
    admitted_t = admitted.T
    queries_t = queries.T
    loads[4].wait()
    stores = []
    step = 64
    for s in range(ROWS):
        total = jnp.zeros((8, HEAD), F32)
        rate = keep[s : s + 1, :]
        value_row = values[s : s + 1, :]
        for r in range(0, HEAD, step):
            block = (
                rate * mem_buf[s, r : r + step, :]
                + admitted_t[r : r + step, s : s + 1] * value_row
            )
            mem_buf[s, r : r + step, :] = block
            weighed = queries_t[r : r + step, s : s + 1] * block
            total = total + jnp.sum(weighed.reshape(step // 8, 8, HEAD), axis=0)
        num_buf[s : s + 1, :] = jnp.sum(total, axis=0, keepdims=True)
        store = pltpu.make_async_copy(mem_buf.at[s], memory_next.at[s, 0], store_sem.at[s])
        store.start()
        stores.append(store)
    out_gate = project(3)
    readout = num_buf[...] / jnp.maximum(jnp.abs(denominator), jnp.exp(-stab))
    mixed = (readout / (1.0 + jnp.exp(-out_gate))).astype(BF16)
    loads[5].wait()
    heads[tp] = jnp.dot(mixed, out_buf[...], preferred_element_type=F32).astype(BF16)

    pl.semaphore_wait(barrier, NEP - 1 + NTP - 1)
    for d in range(1, NTP):
        pltpu.make_async_remote_copy(
            src_ref=heads.at[tp],
            dst_ref=heads.at[tp],
            send_sem=head_sems.at[0],
            recv_sem=head_sems.at[1],
            device_id=(ep, (tp + d) % NTP),
            device_id_type=MESH,
        ).start()

    route_rows = routes[...].astype(F32)
    earlier = iota((ROWS, ROWS), 0) < iota((ROWS, ROWS), 1)
    targets = []
    for choice in range(TOP):
        mine = route_rows[choice : choice + 1, :]
        same = jnp.zeros((ROWS, ROWS), F32)
        for other in range(TOP):
            theirs = column(route_rows[other : other + 1, :], ROWS)
            same = same + jnp.where((theirs == mine) & earlier, 1.0, 0.0)
        targets.append(mine * CAP + jnp.sum(same, axis=0, keepdims=True))
    spread = iota((ROWS, LANES), 1) % ROWS == iota((ROWS, LANES), 0)
    lane_chunk = (iota((1, LANES), 1) // ROWS).astype(F32)
    lane_keys = [
        jnp.sum(jnp.where(spread, column(t, ROWS), 0.0), axis=0, keepdims=True) * CHUNKS
        + lane_chunk
        for t in targets
    ]
    for part in range(8):
        height = NEP * MSG // 8
        row = iota((height, 1), 0) + part * height
        row_key = (
            ((row // MSG) * CAP + row % CAP) * CHUNKS + (row % MSG) // CAP
        ).astype(F32)
        hit = row_key == lane_keys[0]
        for lane_key in lane_keys[1:]:
            hit = hit | (row_key == lane_key)
        pick_buf[part * height : (part + 1) * height, :] = jnp.where(hit, 1.0, 0.0).astype(BF16)
    tall = NTP * ROWS
    copies = iota((tall, ROWS), 0) % ROWS == iota((tall, ROWS), 1)
    tall_chunk = (iota((tall, 1), 0) // ROWS).astype(F32)
    lane = iota((1, NEP * QMSG), 1)
    lane_key = (((lane // QMSG) * CAP + lane % CAP) * QCHUNKS + (lane % QMSG) // CAP).astype(F32)
    weigh = jnp.zeros((tall, NEP * QMSG), F32)
    for choice in range(TOP):
        tall_key = (
            jnp.sum(jnp.where(copies, targets[choice], 0.0), axis=1, keepdims=True) * QCHUNKS
            + tall_chunk
        )
        weight = jnp.sum(
            jnp.where(copies, route_weight[choice : choice + 1, :], 0.0), axis=1, keepdims=True
        )
        weigh = weigh + jnp.where(tall_key == lane_key, weight, 0.0)
    weigh_high = weigh.astype(BF16)
    weigh_low = (weigh - weigh_high.astype(F32)).astype(BF16)

    def arrivals(buffer, count, sems):
        return pltpu.make_async_remote_copy(
            src_ref=buffer.at[pl.ds(0, count)],
            dst_ref=buffer.at[pl.ds(0, count)],
            send_sem=sems.at[0],
            recv_sem=sems.at[1],
            device_id=(ep, tp),
            device_id_type=MESH,
        )

    arrivals(heads, NTP - 1, head_sems).wait_recv()
    summed = heads[0].astype(F32)
    for h in range(1, NTP):
        summed = summed + heads[h].astype(F32)
    residual = token_rows + summed
    for q in range(NTP):
        res_buf[q] = residual[:, q * QUARTER : (q + 1) * QUARTER]
    expert_in = layer_norm(residual, gain_moe[...])

    stacked = jnp.concatenate(
        [expert_in[:, j * LANES : (j + 1) * LANES] for j in range(CHUNKS)], axis=0
    ).astype(BF16)
    for part in range(8):
        height = NEP * MSG // 8
        picked = jnp.dot(
            pick_buf[part * height : (part + 1) * height, :],
            stacked,
            preferred_element_type=F32,
        ).astype(BF16)
        disp_send[part * 8 : (part + 1) * 8] = picked.reshape(8, MSG, LANES)

    def dispatch(k, carry):
        to = partner(ep, k)
        pltpu.make_async_remote_copy(
            src_ref=disp_send.at[to],
            dst_ref=disp_recv.at[ep],
            send_sem=disp_sems.at[0],
            recv_sem=disp_sems.at[1],
            device_id=(to, tp),
            device_id_type=MESH,
        ).start()
        return carry

    lax.fori_loop(0, NEP - 1, dispatch, 0)
    disp_recv[ep] = disp_send[ep]
    for load in loads[6:]:
        load.wait()
    arrivals(disp_recv, NEP - 1, disp_sems).wait_recv()

    for p in range(NEP):
        stage[p * PITCH : p * PITCH + MSG, :] = disp_recv[p].astype(F32)
    gate_up = jnp.zeros((SLOTS, 2 * HIDDEN), F32)
    for j in range(0, CHUNKS, 2):
        wide_rows = jnp.concatenate(
            [
                jnp.concatenate(
                    [stage[pl.ds((j + h) * CAP + c, NEP, stride=PITCH), :] for c in range(CAP)],
                    axis=0,
                )
                for h in range(2)
            ],
            axis=1,
        ).astype(BF16)
        gate_up = gate_up + jnp.dot(
            wide_rows, gu_buf[j * LANES : (j + 2) * LANES, :], preferred_element_type=F32
        )
    gate_part, up_part = gate_up[:, :HIDDEN], gate_up[:, HIDDEN:]
    hidden = (gate_part / (1.0 + jnp.exp(-gate_part)) * up_part).astype(BF16)

    for d in (2, 1, 3):
        to = (tp + d) % NTP
        part_send[d - 1] = jnp.dot(hidden, down_buf[to], preferred_element_type=F32).astype(BF16)
        pltpu.make_async_remote_copy(
            src_ref=part_send.at[d - 1],
            dst_ref=part_recv.at[d - 1],
            send_sem=part_sems.at[0],
            recv_sem=part_sems.at[1],
            device_id=(ep, to),
            device_id_type=MESH,
        ).start()
    own = jnp.dot(hidden, down_buf[tp], preferred_element_type=F32)
    arrivals(part_recv, NTP - 1, part_sems).wait_recv()
    for d in range(NTP - 1):
        own = own + part_recv[d].astype(F32)

    for j in range(QCHUNKS):
        for c in range(CAP):
            ret_stage[pl.ds(j * CAP + c, NEP, stride=QMSG), :] = own[
                c * NEP : (c + 1) * NEP, j * LANES : (j + 1) * LANES
            ]
    ret_send[...] = ret_stage[...].reshape(NEP, QMSG, LANES).astype(BF16)

    def give_back(k, carry):
        to = partner(ep, k)
        pltpu.make_async_remote_copy(
            src_ref=ret_send.at[to],
            dst_ref=ret_recv.at[ep],
            send_sem=ret_sems.at[0],
            recv_sem=ret_sems.at[1],
            device_id=(to, tp),
            device_id_type=MESH,
        ).start()
        return carry

    lax.fori_loop(0, NEP - 1, give_back, 0)
    ret_recv[ep] = ret_send[ep]
    for store in stores:
        store.wait()
    arrivals(heads, NTP - 1, head_sems).wait_send()
    arrivals(disp_recv, NEP - 1, disp_sems).wait_send()
    arrivals(part_recv, NTP - 1, part_sems).wait_send()
    arrivals(ret_recv, NEP - 1, ret_sems).wait_recv()
    returned = ret_recv[...].astype(F32).reshape(NEP * QMSG, LANES).astype(BF16)
    combined = jnp.dot(weigh_high, returned, preferred_element_type=F32) + jnp.dot(
        weigh_low, returned, preferred_element_type=F32
    )
    for j in range(QCHUNKS):
        output[:, j * LANES : (j + 1) * LANES] = (
            res_buf[tp, :, j * LANES : (j + 1) * LANES] + combined[j * ROWS : (j + 1) * ROWS]
        ).astype(BF16)
    arrivals(ret_recv, NEP - 1, ret_sems).wait_send()


def shards(
    tokens,
    w_query,
    w_key,
    w_value,
    w_outgate,
    w_igate,
    w_fgate,
    forget_bias,
    w_out,
    gain_mix,
    gain_moe,
    memory,
    normalizer,
    stabilizer,
    expert_gate,
    expert_up,
    expert_down,
    routes,
    route_weight,
):
    vmem = pl.BlockSpec(memory_space=pltpu.VMEM)
    smem = pl.BlockSpec(memory_space=pltpu.SMEM)
    hbm = pl.BlockSpec(memory_space=pl.ANY)
    output, memory_next, norm_next, stab = pl.pallas_call(
        kernel,
        out_shape=(
            jax.ShapeDtypeStruct((ROWS, QUARTER), BF16),
            jax.ShapeDtypeStruct(memory.shape, F32),
            jax.ShapeDtypeStruct(normalizer.shape, F32),
            jax.ShapeDtypeStruct((1, ROWS), F32),
        ),
        in_specs=[vmem] * 5 + [smem] + [vmem] * 4 + [hbm] * 9,
        out_specs=(vmem, hbm, vmem, vmem),
        scratch_shapes=[
            pltpu.VMEM((4, WIDTH, HEAD), BF16),
            pltpu.VMEM((ROWS, HEAD, HEAD), F32),
            pltpu.VMEM((HEAD, WIDTH), BF16),
            pltpu.VMEM((WIDTH, 2 * HIDDEN), BF16),
            pltpu.VMEM((NTP, HIDDEN, QUARTER), BF16),
            pltpu.VMEM((ROWS, HEAD), F32),
            pltpu.VMEM((NTP, ROWS, QUARTER), F32),
            pltpu.VMEM((NTP, ROWS, WIDTH), BF16),
            pltpu.VMEM((NEP * MSG, LANES), BF16),
            pltpu.VMEM((NEP * PITCH, LANES), F32),
            pltpu.VMEM((NEP, MSG, LANES), BF16),
            pltpu.VMEM((NEP, MSG, LANES), BF16),
            pltpu.VMEM((NTP - 1, SLOTS, QUARTER), BF16),
            pltpu.VMEM((NTP - 1, SLOTS, QUARTER), BF16),
            pltpu.VMEM((NEP * QMSG, LANES), F32),
            pltpu.VMEM((NEP, QMSG, LANES), BF16),
            pltpu.VMEM((NEP, QMSG, LANES), BF16),
            pltpu.SemaphoreType.DMA((12,)),
            pltpu.SemaphoreType.DMA((ROWS,)),
            pltpu.SemaphoreType.DMA((2,)),
            pltpu.SemaphoreType.DMA((2,)),
            pltpu.SemaphoreType.DMA((2,)),
            pltpu.SemaphoreType.DMA((2,)),
        ],
        compiler_params=pltpu.CompilerParams(
            collective_id=0, has_side_effects=True, vmem_limit_bytes=60 * 1024 * 1024
        ),
        name="layer",
    )(
        tokens,
        gain_mix.reshape(1, WIDTH),
        gain_moe.reshape(1, WIDTH),
        w_igate.reshape(1, WIDTH),
        w_fgate.reshape(1, WIDTH),
        forget_bias,
        normalizer,
        stabilizer.reshape(1, ROWS),
        routes.T,
        route_weight.T,
        w_key,
        w_value,
        w_query,
        w_outgate,
        memory,
        w_out,
        expert_gate,
        expert_up,
        expert_down,
    )
    return output, memory_next, norm_next, stab.reshape(ROWS, 1)


def solution(mesh):
    return jax.shard_map(
        shards,
        mesh=mesh,
        in_specs=(
            P("ep", None),
            P(None, "tp"),
            P(None, "tp"),
            P(None, "tp"),
            P(None, "tp"),
            P(None, "tp"),
            P(None, "tp"),
            P("tp"),
            P("tp", None),
            P(),
            P(),
            P("ep", "tp", None, None),
            P("ep", "tp", None),
            P("ep", "tp"),
            P("ep", None, "tp"),
            P("ep", None, "tp"),
            P("ep", "tp", None),
            P("ep", None),
            P("ep", None),
        ),
        out_specs=(P("ep", "tp"), P("ep", "tp", None, None), P("ep", "tp", None), P("ep", "tp")),
        check_vma=False,
    )
```

```python
import functools

import jax
import jax.numpy as jnp
from jax import lax
from jax.experimental import pallas as pl
from jax.experimental.pallas import tpu as pltpu
from jax.sharding import PartitionSpec as P

F32 = jnp.float32
BF16 = jnp.bfloat16
MESH = pl.DeviceIdType.MESH

ROWS = 8
WIDTH = 2048
HEAD = 256
HIDDEN = 128
TOP = 4
NEP = 64
NTP = 4
CAP = 2
SLOTS = NEP * CAP
LANES = 128
QUARTER = WIDTH // NTP
QCHUNKS = QUARTER // LANES
QMSG = QCHUNKS * CAP
HALF = NEP // 2


def layer_norm(values, gain):
    mean = jnp.mean(values, -1, keepdims=True)
    centered = values - mean
    variance = jnp.mean(centered * centered, -1, keepdims=True)
    return centered * lax.rsqrt(variance + 1e-05) * gain


def iota(shape, dim):
    return lax.broadcasted_iota(jnp.int32, shape, dim)


def column(row, size):
    eye = iota((size, size), 0) == iota((size, size), 1)
    return jnp.sum(jnp.where(eye, row, 0.0), axis=1, keepdims=True)


def ring_step(k, middle):
    return middle + (k // 2) * (1 - 2 * (k % 2)) - k % 2


def each_partner(ep, sign, first, last, act):
    z, y, c = ep // 8, (ep // 2) % 4, ep % 2
    columns = [
        ((y + sign * ring_step(m, 2) + 4) % 4) * 2 + (c + sign * dc + 2) % 2
        for m in range(4)
        for dc in (1, 0)
    ]

    def plane(a, count):
        base = ((z + sign * ring_step(a, 4) + 8) % 8) * 8
        for b in range(count):
            act(a * 8 + b, base + columns[b])

    def whole(a, carry):
        plane(a, 8)
        return carry

    if last == NEP:
        lax.fori_loop(first // 8, last // 8 - 1, whole, 0)
        plane(NEP // 8 - 1, 7)
    else:
        lax.fori_loop(first // 8, last // 8, whole, 0)


def kernel(
    tokens_in,
    gain_mix_in,
    gain_moe_in,
    w_igate_in,
    w_fgate_in,
    normalizer_in,
    stabilizer_in,
    routes_in,
    route_weight_in,
    w_key,
    w_value,
    w_query,
    w_outgate,
    memory,
    w_out,
    expert_gate,
    expert_up,
    expert_down,
    forget_bias,
    output,
    admitted_out,
    values_out,
    keep_out,
    norm_next,
    stabilizer_next,
    tokens,
    gain_mix,
    gain_moe,
    w_igate,
    w_fgate,
    normalizer,
    stabilizer,
    routes,
    route_weight,
    w_buf,
    mem_buf,
    out_buf,
    gu_buf,
    down_buf,
    num_buf,
    res_buf,
    in_buf,
    heads,
    stage,
    disp_send,
    rows,
    part_send,
    part_recv,
    ret_stage,
    ret_send,
    ret_recv,
    small_sem,
    load_sem,
    head_sems,
    disp_sems,
    row_sems,
    part_sems,
    ret_sems,
):
    ep = lax.axis_index("ep")
    tp = lax.axis_index("tp")

    smalls = [
        pltpu.make_async_copy(source, target, small_sem.at[i])
        for i, (source, target) in enumerate(
            (
                (tokens_in, tokens),
                (gain_mix_in, gain_mix),
                (w_igate_in, w_igate),
                (w_fgate_in, w_fgate),
                (stabilizer_in, stabilizer),
                (normalizer_in, normalizer),
                (gain_moe_in, gain_moe),
                (routes_in, routes),
                (route_weight_in, route_weight),
            )
        )
    ]
    loads = [
        pltpu.make_async_copy(w, w_buf.at[i], load_sem.at[i])
        for i, w in enumerate((w_key, w_value, w_query, w_outgate))
    ]
    loads.append(pltpu.make_async_copy(memory.at[:, 0], mem_buf, load_sem.at[4]))
    loads.append(pltpu.make_async_copy(w_out, out_buf, load_sem.at[5]))
    loads.append(
        pltpu.make_async_copy(expert_gate.at[0], gu_buf.at[:, pl.ds(0, HIDDEN)], load_sem.at[6])
    )
    loads.append(
        pltpu.make_async_copy(
            expert_up.at[0], gu_buf.at[:, pl.ds(HIDDEN, HIDDEN)], load_sem.at[7]
        )
    )
    for q in range(NTP):
        loads.append(
            pltpu.make_async_copy(
                expert_down.at[0, :, pl.ds(q * QUARTER, QUARTER)],
                down_buf.at[q],
                load_sem.at[8 + q],
            )
        )
    for load in smalls + loads:
        load.start()

    barrier = pltpu.get_barrier_semaphore()

    def greet(k, index):
        pl.semaphore_signal(barrier, inc=1, device_id=(index, tp), device_id_type=MESH)

    each_partner(ep, 1, 0, NEP, greet)
    for d in range(1, NTP):
        pl.semaphore_signal(
            barrier, inc=1, device_id=(ep, (tp + d) % NTP), device_id_type=MESH
        )

    for small in smalls[:6]:
        small.wait()
    token_rows = tokens[...].astype(F32)
    normed = layer_norm(token_rows, gain_mix[...]).astype(BF16)
    wide = normed.astype(F32)
    gate_in = jnp.sum(wide * w_igate[...].astype(F32), axis=1, keepdims=True)
    gate_forget = jnp.sum(wide * w_fgate[...].astype(F32), axis=1, keepdims=True)
    shifted = gate_forget + forget_bias[0]
    log_forget = jnp.minimum(shifted, 0.0) - jnp.log1p(jnp.exp(-jnp.abs(shifted)))
    carried = log_forget + column(stabilizer[...], ROWS)
    stab = jnp.maximum(carried, gate_in)
    keep = jnp.exp(carried - stab)
    admit = jnp.exp(gate_in - stab)
    eye = iota((ROWS, ROWS), 0) == iota((ROWS, ROWS), 1)
    stabilizer_next[...] = jnp.sum(jnp.where(eye, stab, 0.0), axis=0, keepdims=True)

    def project(i):
        loads[i].wait()
        product = jnp.dot(normed, w_buf[i], preferred_element_type=F32)
        return product.astype(BF16).astype(F32)

    keys = project(0) * (1.0 / 16.0)
    values = project(1)
    queries = project(2)
    admitted = admit * keys
    new_norm = keep * normalizer[:, 0, :] + admitted
    norm_next[:, 0, :] = new_norm
    admitted_out[...] = admitted
    values_out[...] = values
    keep_out[...] = jnp.broadcast_to(keep, (ROWS, LANES))
    denominator = jnp.sum(queries * new_norm, axis=1, keepdims=True)
    admitted_t = admitted.T
    queries_t = queries.T
    loads[4].wait()
    step = 64
    for s in range(ROWS):
        total = jnp.zeros((8, HEAD), F32)
        rate = keep[s : s + 1, :]
        value_row = values[s : s + 1, :]
        for r in range(0, HEAD, step):
            block = (
                rate * mem_buf[s, r : r + step, :]
                + admitted_t[r : r + step, s : s + 1] * value_row
            )
            weighed = queries_t[r : r + step, s : s + 1] * block
            total = total + jnp.sum(weighed.reshape(step // 8, 8, HEAD), axis=0)
        num_buf[s : s + 1, :] = jnp.sum(total, axis=0, keepdims=True)
    out_gate = project(3)
    readout = num_buf[...] / jnp.maximum(jnp.abs(denominator), jnp.exp(-stab))
    mixed = (readout / (1.0 + jnp.exp(-out_gate))).astype(BF16)
    loads[5].wait()
    heads[tp] = jnp.dot(mixed, out_buf[...], preferred_element_type=F32).astype(BF16)

    pl.semaphore_wait(barrier, NEP - 1 + NTP - 1)
    for d in (2, 1, 3):
        pltpu.make_async_remote_copy(
            src_ref=heads.at[tp],
            dst_ref=heads.at[tp],
            send_sem=head_sems.at[0],
            recv_sem=head_sems.at[1],
            device_id=(ep, (tp + d) % NTP),
            device_id_type=MESH,
        ).start()

    for small in smalls[6:]:
        small.wait()
    route_rows = routes[...].astype(F32)
    earlier = iota((ROWS, ROWS), 0) < iota((ROWS, ROWS), 1)
    targets = []
    for choice in range(TOP):
        mine = route_rows[choice : choice + 1, :]
        same = jnp.zeros((ROWS, ROWS), F32)
        for other in range(TOP):
            theirs = column(route_rows[other : other + 1, :], ROWS)
            same = same + jnp.where((theirs == mine) & earlier, 1.0, 0.0)
        targets.append(mine * CAP + jnp.sum(same, axis=0, keepdims=True))
    tall = QCHUNKS * ROWS
    copies = iota((tall, ROWS), 0) % ROWS == iota((tall, ROWS), 1)
    tall_chunk = (iota((tall, 1), 0) // ROWS).astype(F32)
    lane = iota((1, NEP * QMSG), 1)
    lane_key = (((lane // QMSG) * CAP + lane % CAP) * QCHUNKS + (lane % QMSG) // CAP).astype(F32)
    weigh = jnp.zeros((tall, NEP * QMSG), F32)
    filled = jnp.zeros((tall, NEP * QMSG), F32)
    for choice in range(TOP):
        tall_key = (
            jnp.sum(jnp.where(copies, targets[choice], 0.0), axis=1, keepdims=True) * QCHUNKS
            + tall_chunk
        )
        weight = jnp.sum(
            jnp.where(copies, route_weight[choice : choice + 1, :], 0.0), axis=1, keepdims=True
        )
        hit = tall_key == lane_key
        weigh = weigh + jnp.where(hit, weight, 0.0)
        filled = filled + jnp.where(hit, 1.0, 0.0)
    weigh_high = weigh.astype(BF16)
    weigh_low = (weigh - weigh_high.astype(F32)).astype(BF16)
    pick = filled.T.astype(BF16)

    def bytes_of(view, sems):
        return pltpu.make_async_remote_copy(
            src_ref=view,
            dst_ref=view,
            send_sem=sems.at[0],
            recv_sem=sems.at[1],
            device_id=(ep, tp),
            device_id_type=MESH,
        )

    bytes_of(heads.at[pl.ds(0, NTP - 1)], head_sems).wait_recv()
    summed = heads[0].astype(F32)
    for h in range(1, NTP):
        summed = summed + heads[h].astype(F32)
    residual = token_rows + summed
    expert_in = layer_norm(residual, gain_moe[...])
    for q in range(NTP):
        res_buf[q] = residual[:, q * QUARTER : (q + 1) * QUARTER]
        in_buf[q] = expert_in[:, q * QUARTER : (q + 1) * QUARTER]

    stacked = jnp.concatenate(
        [in_buf[tp, :, j * LANES : (j + 1) * LANES] for j in range(QCHUNKS)], axis=0
    ).astype(BF16)
    picked = jnp.dot(pick, stacked, preferred_element_type=F32).astype(BF16)
    disp_send[...] = picked.reshape(NEP, QMSG, LANES)

    def dispatch(group):
        def send(k, to):
            pltpu.make_async_remote_copy(
                src_ref=disp_send.at[to],
                dst_ref=rows.at[tp, k],
                send_sem=disp_sems.at[group, 0],
                recv_sem=disp_sems.at[group, 1],
                device_id=(to, tp),
                device_id_type=MESH,
            ).start()

        each_partner(ep, 1, group * HALF, (group + 1) * HALF, send)

    dispatch(0)
    dispatch(1)
    rows[tp, NEP - 1] = disp_send[ep]

    def spread(group):
        block = pl.ds(group * HALF, HALF)
        bytes_of(
            rows.at[0, pl.ds(group * HALF, HALF - group)], disp_sems.at[group]
        ).wait_recv()
        for d in (2, 1, 3):
            pltpu.make_async_remote_copy(
                src_ref=rows.at[tp, block],
                dst_ref=rows.at[tp, block],
                send_sem=row_sems.at[group, 0],
                recv_sem=row_sems.at[group, 1],
                device_id=(ep, (tp + d) % NTP),
                device_id_type=MESH,
            ).start()

    def spread_bytes(group):
        return bytes_of(
            rows.at[pl.ds(0, NTP - 1), pl.ds(group * HALF, HALF)], row_sems.at[group]
        )

    def expert(group):
        spread_bytes(group).wait_recv()
        height = HALF * QMSG
        for q in range(NTP):
            stage[q * height : (q + 1) * height, :] = (
                rows[q, group * HALF : (group + 1) * HALF].astype(F32).reshape(height, LANES)
            )
        gate_up = jnp.zeros((HALF * CAP, 2 * HIDDEN), F32)
        for q in range(NTP):
            for j in range(0, QCHUNKS, 2):
                wide_rows = jnp.concatenate(
                    [
                        jnp.concatenate(
                            [
                                stage[
                                    pl.ds(q * height + (j + h) * CAP + c, HALF, stride=QMSG), :
                                ]
                                for c in range(CAP)
                            ],
                            axis=0,
                        )
                        for h in range(2)
                    ],
                    axis=1,
                ).astype(BF16)
                first = q * QUARTER + j * LANES
                gate_up = gate_up + jnp.dot(
                    wide_rows, gu_buf[first : first + 2 * LANES, :], preferred_element_type=F32
                )
        gate_part, up_part = gate_up[:, :HIDDEN], gate_up[:, HIDDEN:]
        hidden = (gate_part / (1.0 + jnp.exp(-gate_part)) * up_part).astype(BF16)
        for d in (2, 1, 3):
            to = (tp + d) % NTP
            part_send[group, d - 1] = jnp.dot(
                hidden, down_buf[to], preferred_element_type=F32
            ).astype(BF16)
            pltpu.make_async_remote_copy(
                src_ref=part_send.at[group, d - 1],
                dst_ref=part_recv.at[group, d - 1],
                send_sem=part_sems.at[group, 0],
                recv_sem=part_sems.at[group, 1],
                device_id=(ep, to),
                device_id_type=MESH,
            ).start()
        return jnp.dot(hidden, down_buf[tp], preferred_element_type=F32)

    def give_back(group, own):
        bytes_of(part_recv.at[group], part_sems.at[group]).wait_recv()
        for d in range(NTP - 1):
            own = own + part_recv[group, d].astype(F32)
        for j in range(QCHUNKS):
            for c in range(CAP):
                ret_stage[pl.ds(j * CAP + c, HALF, stride=QMSG), :] = own[
                    c * HALF : (c + 1) * HALF, j * LANES : (j + 1) * LANES
                ]
        ret_send[group * HALF : (group + 1) * HALF] = (
            ret_stage[...].reshape(HALF, QMSG, LANES).astype(BF16)
        )

        def send(k, to):
            pltpu.make_async_remote_copy(
                src_ref=ret_send.at[k],
                dst_ref=ret_recv.at[ep],
                send_sem=ret_sems.at[0],
                recv_sem=ret_sems.at[1],
                device_id=(to, tp),
                device_id_type=MESH,
            ).start()

        each_partner(ep, -1, group * HALF, (group + 1) * HALF, send)

    spread(1)
    spread(0)
    for load in loads[6:]:
        load.wait()
    near = expert(1)
    far = expert(0)
    give_back(1, near)
    give_back(0, far)
    ret_recv[ep] = ret_send[NEP - 1]
    bytes_of(heads.at[pl.ds(0, NTP - 1)], head_sems).wait_send()
    for group in range(2):
        bytes_of(
            rows.at[0, pl.ds(group * HALF, HALF - group)], disp_sems.at[group]
        ).wait_send()
        spread_bytes(group).wait_send()
        bytes_of(part_recv.at[group], part_sems.at[group]).wait_send()
    everything = bytes_of(ret_recv.at[pl.ds(0, NEP - 1)], ret_sems)
    everything.wait_recv()
    returned = ret_recv[...].astype(F32).reshape(NEP * QMSG, LANES).astype(BF16)
    combined = jnp.dot(weigh_high, returned, preferred_element_type=F32) + jnp.dot(
        weigh_low, returned, preferred_element_type=F32
    )
    for j in range(QCHUNKS):
        output[:, j * LANES : (j + 1) * LANES] = (
            res_buf[tp, :, j * LANES : (j + 1) * LANES] + combined[j * ROWS : (j + 1) * ROWS]
        ).astype(BF16)
    everything.wait_send()


def update_kernel(
    admitted_in,
    values_in,
    keep_in,
    memory,
    output_in,
    norm_in,
    stab_in,
    memory_next,
    output,
    norm_next,
    stabilizer_next,
    admitted,
    values,
    keep,
    mem_buf,
    output_buf,
    norm_buf,
    stab_buf,
    load_sem,
    store_sem,
):
    loads = [
        pltpu.make_async_copy(source, target, load_sem.at[i])
        for i, (source, target) in enumerate(
            (
                (admitted_in, admitted),
                (values_in, values),
                (keep_in, keep),
                (output_in, output_buf),
                (norm_in, norm_buf),
                (stab_in, stab_buf),
            )
        )
    ]
    blocks = [
        pltpu.make_async_copy(memory.at[s, 0], mem_buf.at[s], load_sem.at[6 + s])
        for s in range(ROWS)
    ]
    for load in loads + blocks:
        load.start()
    passed = [
        pltpu.make_async_copy(source, target, store_sem.at[ROWS + i])
        for i, (source, target) in enumerate(
            ((output_buf, output), (norm_buf, norm_next), (stab_buf, stabilizer_next))
        )
    ]
    for load in loads[:3]:
        load.wait()
    admitted_t = admitted[...].T
    for load, store in zip(loads[3:], passed, strict=True):
        load.wait()
        store.start()
    stores = []
    for s in range(ROWS):
        blocks[s].wait()
        mem_buf[s] = (
            keep[s : s + 1, 0:1] * mem_buf[s] + admitted_t[:, s : s + 1] * values[s : s + 1, :]
        )
        store = pltpu.make_async_copy(mem_buf.at[s], memory_next.at[s, 0], store_sem.at[s])
        store.start()
        stores.append(store)
    for store in passed + stores:
        store.wait()


def shards(
    tokens,
    w_query,
    w_key,
    w_value,
    w_outgate,
    w_igate,
    w_fgate,
    forget_bias,
    w_out,
    gain_mix,
    gain_moe,
    memory,
    normalizer,
    stabilizer,
    expert_gate,
    expert_up,
    expert_down,
    routes,
    route_weight,
):
    vmem = pl.BlockSpec(memory_space=pltpu.VMEM)
    smem = pl.BlockSpec(memory_space=pltpu.SMEM)
    hbm = pl.BlockSpec(memory_space=pl.ANY)
    smalls = (
        tokens,
        gain_mix.reshape(1, WIDTH),
        gain_moe.reshape(1, WIDTH),
        w_igate.reshape(1, WIDTH),
        w_fgate.reshape(1, WIDTH),
        normalizer,
        stabilizer.reshape(1, ROWS),
        routes.T,
        route_weight.T,
    )
    norm_shape = jax.ShapeDtypeStruct(normalizer.shape, F32)
    output_shape = jax.ShapeDtypeStruct((ROWS, QUARTER), BF16)
    stab_shape = jax.ShapeDtypeStruct((1, ROWS), F32)
    row_shape = jax.ShapeDtypeStruct((ROWS, HEAD), F32)
    keep_shape = jax.ShapeDtypeStruct((ROWS, LANES), F32)
    message = (QMSG, LANES)
    output, admitted, values, keep, norm_next, stab = pl.pallas_call(
        kernel,
        out_shape=(output_shape, row_shape, row_shape, keep_shape, norm_shape, stab_shape),
        in_specs=[hbm] * 18 + [smem],
        out_specs=(vmem,) * 6,
        scratch_shapes=[pltpu.VMEM(x.shape, x.dtype) for x in smalls]
        + [
            pltpu.VMEM((4, WIDTH, HEAD), BF16),
            pltpu.VMEM((ROWS, HEAD, HEAD), F32),
            pltpu.VMEM((HEAD, WIDTH), BF16),
            pltpu.VMEM((WIDTH, 2 * HIDDEN), BF16),
            pltpu.VMEM((NTP, HIDDEN, QUARTER), BF16),
            pltpu.VMEM((ROWS, HEAD), F32),
            pltpu.VMEM((NTP, ROWS, QUARTER), F32),
            pltpu.VMEM((NTP, ROWS, QUARTER), F32),
            pltpu.VMEM((NTP, ROWS, WIDTH), BF16),
            pltpu.VMEM((NTP * HALF * QMSG, LANES), F32),
            pltpu.VMEM((NEP, *message), BF16),
            pltpu.VMEM((NTP, NEP, *message), BF16),
            pltpu.VMEM((2, NTP - 1, HALF * CAP, QUARTER), BF16),
            pltpu.VMEM((2, NTP - 1, HALF * CAP, QUARTER), BF16),
            pltpu.VMEM((HALF * QMSG, LANES), F32),
            pltpu.VMEM((NEP, *message), BF16),
            pltpu.VMEM((NEP, *message), BF16),
            pltpu.SemaphoreType.DMA((9,)),
            pltpu.SemaphoreType.DMA((12,)),
            pltpu.SemaphoreType.DMA((2,)),
            pltpu.SemaphoreType.DMA((2, 2)),
            pltpu.SemaphoreType.DMA((2, 2)),
            pltpu.SemaphoreType.DMA((2, 2)),
            pltpu.SemaphoreType.DMA((2,)),
        ],
        compiler_params=pltpu.CompilerParams(
            collective_id=0, has_side_effects=True, vmem_limit_bytes=60 * 1024 * 1024
        ),
        name="layer",
    )(
        *smalls,
        w_key,
        w_value,
        w_query,
        w_outgate,
        memory,
        w_out,
        expert_gate,
        expert_up,
        expert_down,
        forget_bias,
    )
    memory_next, output, norm_next, stab = pl.pallas_call(
        update_kernel,
        out_shape=(
            jax.ShapeDtypeStruct(memory.shape, F32),
            output_shape,
            norm_shape,
            stab_shape,
        ),
        in_specs=[hbm] * 7,
        out_specs=(hbm,) * 4,
        scratch_shapes=[
            pltpu.VMEM((ROWS, HEAD), F32),
            pltpu.VMEM((ROWS, HEAD), F32),
            pltpu.VMEM((ROWS, LANES), F32),
            pltpu.VMEM((ROWS, HEAD, HEAD), F32),
            pltpu.VMEM(output_shape.shape, BF16),
            pltpu.VMEM(norm_shape.shape, F32),
            pltpu.VMEM(stab_shape.shape, F32),
            pltpu.SemaphoreType.DMA((6 + ROWS,)),
            pltpu.SemaphoreType.DMA((ROWS + 3,)),
        ],
        compiler_params=pltpu.CompilerParams(vmem_limit_bytes=60 * 1024 * 1024),
        name="update",
    )(admitted, values, keep, memory, output, norm_next, stab)
    return output, memory_next, norm_next, stab.reshape(ROWS, 1)


def solution(mesh):
    return jax.shard_map(
        shards,
        mesh=mesh,
        in_specs=(
            P("ep", None),
            P(None, "tp"),
            P(None, "tp"),
            P(None, "tp"),
            P(None, "tp"),
            P(None, "tp"),
            P(None, "tp"),
            P("tp"),
            P("tp", None),
            P(),
            P(),
            P("ep", "tp", None, None),
            P("ep", "tp", None),
            P("ep", "tp"),
            P("ep", None, "tp"),
            P("ep", None, "tp"),
            P("ep", "tp", None),
            P("ep", None),
            P("ep", None),
        ),
        out_specs=(P("ep", "tp"), P("ep", "tp", None, None), P("ep", "tp", None), P("ep", "tp")),
        check_vma=False,
    )
```

```python
import functools

import jax
import jax.numpy as jnp
from jax import lax
from jax.experimental import pallas as pl
from jax.experimental.pallas import tpu as pltpu
from jax.sharding import PartitionSpec as P

F32 = jnp.float32
BF16 = jnp.bfloat16
MESH = pl.DeviceIdType.MESH

ROWS = 8
WIDTH = 2048
HEAD = 256
HIDDEN = 128
TOP = 4
NEP = 64
NTP = 4
CAP = 2
SLOTS = NEP * CAP
LANES = 128
QUARTER = WIDTH // NTP
QCHUNKS = QUARTER // LANES
QMSG = QCHUNKS * CAP
GROUPS = 4
GROUP = NEP // GROUPS


def layer_norm(values, gain):
    mean = jnp.mean(values, -1, keepdims=True)
    centered = values - mean
    variance = jnp.mean(centered * centered, -1, keepdims=True)
    return centered * lax.rsqrt(variance + 1e-05) * gain


def iota(shape, dim):
    return lax.broadcasted_iota(jnp.int32, shape, dim)


def column(row, size):
    eye = iota((size, size), 0) == iota((size, size), 1)
    return jnp.sum(jnp.where(eye, row, 0.0), axis=1, keepdims=True)


def ring_step(k):
    return (k // 2) * (1 - 2 * (k % 2)) - k % 2


def each_partner(ep, sign, first, last, act, far_first=False):
    z, y, c = ep // 8, (ep // 2) % 4, ep % 2
    columns = [
        ((y + sign * ring_step(m) + 4) % 4) * 2 + (c + sign * dc + 2) % 2
        for m in range(4)
        for dc in (0, 1)
    ]
    low, high = max(first // 8, 1), last // 8

    def plane(a, start):
        base = ((z + sign * ring_step(a) + 8) % 8) * 8
        order = range(7, start - 1, -1) if far_first else range(start, 8)
        for b in order:
            act(a * 8 + b, base + columns[b])

    def whole(i, carry):
        plane(low + high - 1 - i if far_first else i, 0)
        return carry

    if first == 0 and not far_first:
        plane(0, 1)
    lax.fori_loop(low, high, whole, 0)
    if first == 0 and far_first:
        plane(0, 1)


def kernel(
    tokens_in,
    gain_mix_in,
    gain_moe_in,
    w_igate_in,
    w_fgate_in,
    normalizer_in,
    stabilizer_in,
    routes_in,
    route_weight_in,
    w_key,
    w_value,
    w_query,
    w_outgate,
    memory,
    w_out,
    expert_gate,
    expert_up,
    expert_down,
    forget_bias,
    output,
    admitted_out,
    values_out,
    keep_out,
    norm_next,
    stabilizer_next,
    tokens,
    gain_mix,
    gain_moe,
    w_igate,
    w_fgate,
    normalizer,
    stabilizer,
    routes,
    route_weight,
    w_buf,
    mem_buf,
    out_buf,
    gu_buf,
    down_buf,
    num_buf,
    res_buf,
    in_buf,
    heads,
    stage,
    disp_send,
    disp_opposite,
    rows,
    part_send,
    part_recv,
    ret_stage,
    ret_send,
    ret_recv,
    small_sem,
    load_sem,
    head_sems,
    disp_sems,
    row_sems,
    part_sems,
    ret_sems,
):
    ep = lax.axis_index("ep")
    tp = lax.axis_index("tp")

    smalls = [
        pltpu.make_async_copy(source, target, small_sem.at[i])
        for i, (source, target) in enumerate(
            (
                (tokens_in, tokens),
                (gain_mix_in, gain_mix),
                (w_igate_in, w_igate),
                (w_fgate_in, w_fgate),
                (stabilizer_in, stabilizer),
                (normalizer_in, normalizer),
                (gain_moe_in, gain_moe),
                (routes_in, routes),
                (route_weight_in, route_weight),
            )
        )
    ]
    loads = [
        pltpu.make_async_copy(w, w_buf.at[i], load_sem.at[i])
        for i, w in enumerate((w_key, w_value, w_query, w_outgate))
    ]
    loads.append(pltpu.make_async_copy(memory.at[:, 0], mem_buf, load_sem.at[4]))
    loads.append(pltpu.make_async_copy(w_out, out_buf, load_sem.at[5]))
    loads.append(
        pltpu.make_async_copy(expert_gate, gu_buf.at[:, :, pl.ds(0, HIDDEN)], load_sem.at[6])
    )
    loads.append(
        pltpu.make_async_copy(
            expert_up, gu_buf.at[:, :, pl.ds(HIDDEN, HIDDEN)], load_sem.at[7]
        )
    )
    for q in range(NTP):
        loads.append(
            pltpu.make_async_copy(
                expert_down.at[0, :, pl.ds(q * QUARTER, QUARTER)],
                down_buf.at[q],
                load_sem.at[8 + q],
            )
        )
    for small in smalls:
        small.start()

    barrier = pltpu.get_barrier_semaphore()
    opposite = (tp + 2) % NTP

    def greet(k, index):
        pl.semaphore_signal(barrier, inc=1, device_id=(index, tp), device_id_type=MESH)

    each_partner(ep, 1, NEP // 2, NEP, greet, far_first=True)
    for i in (0, 1, 2, 4, 3, 5):
        loads[i].start()
    each_partner(ep, 1, 0, NEP // 2, greet, far_first=True)
    for d in range(1, NTP):
        pl.semaphore_signal(
            barrier, inc=1, device_id=(ep, (tp + d) % NTP), device_id_type=MESH
        )

    for small in smalls[:6]:
        small.wait()
    token_rows = tokens[...].astype(F32)
    normed = layer_norm(token_rows, gain_mix[...]).astype(BF16)
    wide = normed.astype(F32)
    gate_in = jnp.sum(wide * w_igate[...].astype(F32), axis=1, keepdims=True)
    gate_forget = jnp.sum(wide * w_fgate[...].astype(F32), axis=1, keepdims=True)
    shifted = gate_forget + forget_bias[0]
    log_forget = jnp.minimum(shifted, 0.0) - jnp.log1p(jnp.exp(-jnp.abs(shifted)))
    carried = log_forget + column(stabilizer[...], ROWS)
    stab = jnp.maximum(carried, gate_in)
    keep = jnp.exp(carried - stab)
    admit = jnp.exp(gate_in - stab)
    eye = iota((ROWS, ROWS), 0) == iota((ROWS, ROWS), 1)
    stabilizer_next[...] = jnp.sum(jnp.where(eye, stab, 0.0), axis=0, keepdims=True)

    def project(i):
        loads[i].wait()
        product = jnp.dot(normed, w_buf[i], preferred_element_type=F32)
        return product.astype(BF16).astype(F32)

    keys = project(0) * (1.0 / 16.0)
    values = project(1)
    queries = project(2)
    admitted = admit * keys
    new_norm = keep * normalizer[:, 0, :] + admitted
    norm_next[:, 0, :] = new_norm
    admitted_out[...] = admitted
    values_out[...] = values
    keep_out[...] = jnp.broadcast_to(keep, (ROWS, LANES))
    denominator = jnp.sum(queries * new_norm, axis=1, keepdims=True)
    admitted_t = admitted.T
    queries_t = queries.T
    loads[4].wait()
    step = 64
    for s in range(ROWS):
        total = jnp.zeros((8, HEAD), F32)
        rate = keep[s : s + 1, :]
        value_row = values[s : s + 1, :]
        for r in range(0, HEAD, step):
            block = (
                rate * mem_buf[s, r : r + step, :]
                + admitted_t[r : r + step, s : s + 1] * value_row
            )
            weighed = queries_t[r : r + step, s : s + 1] * block
            total = total + jnp.sum(weighed.reshape(step // 8, 8, HEAD), axis=0)
        num_buf[s : s + 1, :] = jnp.sum(total, axis=0, keepdims=True)
    out_gate = project(3)
    readout = num_buf[...] / jnp.maximum(jnp.abs(denominator), jnp.exp(-stab))
    mixed = (readout / (1.0 + jnp.exp(-out_gate))).astype(BF16)
    loads[5].wait()
    heads[tp] = jnp.dot(mixed, out_buf[...], preferred_element_type=F32).astype(BF16)

    pl.semaphore_wait(barrier, NEP - 1 + NTP - 1)
    for d in (2, 1, 3):
        pltpu.make_async_remote_copy(
            src_ref=heads.at[tp],
            dst_ref=heads.at[tp],
            send_sem=head_sems.at[0],
            recv_sem=head_sems.at[1],
            device_id=(ep, (tp + d) % NTP),
            device_id_type=MESH,
        ).start()

    for load in loads[6:]:
        load.start()

    for small in smalls[6:]:
        small.wait()
    route_rows = routes[...].astype(F32)
    earlier = iota((ROWS, ROWS), 0) < iota((ROWS, ROWS), 1)
    targets = []
    for choice in range(TOP):
        mine = route_rows[choice : choice + 1, :]
        same = jnp.zeros((ROWS, ROWS), F32)
        for other in range(TOP):
            theirs = column(route_rows[other : other + 1, :], ROWS)
            same = same + jnp.where((theirs == mine) & earlier, 1.0, 0.0)
        targets.append(mine * CAP + jnp.sum(same, axis=0, keepdims=True))
    tall = QCHUNKS * ROWS
    copies = iota((tall, ROWS), 0) % ROWS == iota((tall, ROWS), 1)
    tall_chunk = (iota((tall, 1), 0) // ROWS).astype(F32)
    lane = iota((1, NEP * QMSG), 1)
    lane_key = (((lane // QMSG) * CAP + lane % CAP) * QCHUNKS + (lane % QMSG) // CAP).astype(F32)
    weigh = jnp.zeros((tall, NEP * QMSG), F32)
    filled = jnp.zeros((tall, NEP * QMSG), F32)
    for choice in range(TOP):
        tall_key = (
            jnp.sum(jnp.where(copies, targets[choice], 0.0), axis=1, keepdims=True) * QCHUNKS
            + tall_chunk
        )
        weight = jnp.sum(
            jnp.where(copies, route_weight[choice : choice + 1, :], 0.0), axis=1, keepdims=True
        )
        hit = tall_key == lane_key
        weigh = weigh + jnp.where(hit, weight, 0.0)
        filled = filled + jnp.where(hit, 1.0, 0.0)
    weigh_high = weigh.astype(BF16)
    weigh_low = (weigh - weigh_high.astype(F32)).astype(BF16)
    pick = filled.T.astype(BF16)

    def bytes_of(view, sems):
        return pltpu.make_async_remote_copy(
            src_ref=view,
            dst_ref=view,
            send_sem=sems.at[0],
            recv_sem=sems.at[1],
            device_id=(ep, tp),
            device_id_type=MESH,
        )

    bytes_of(heads.at[pl.ds(0, NTP - 1)], head_sems).wait_recv()
    summed = heads[0].astype(F32)
    for h in range(1, NTP):
        summed = summed + heads[h].astype(F32)
    residual = token_rows + summed
    expert_in = layer_norm(residual, gain_moe[...])
    for q in range(NTP):
        res_buf[q] = residual[:, q * QUARTER : (q + 1) * QUARTER]
        in_buf[q] = expert_in[:, q * QUARTER : (q + 1) * QUARTER]

    def pick_quarter(q):
        stacked = jnp.concatenate(
            [in_buf[q, :, j * LANES : (j + 1) * LANES] for j in range(QCHUNKS)], axis=0
        ).astype(BF16)
        picked = jnp.dot(pick, stacked, preferred_element_type=F32).astype(BF16)
        return picked.reshape(NEP, QMSG, LANES)

    def dispatch(first, last, source, q, sems, far_first):
        def send(k, to):
            pltpu.make_async_remote_copy(
                src_ref=source.at[to],
                dst_ref=rows.at[q, k],
                send_sem=sems.at[0],
                recv_sem=sems.at[1],
                device_id=(to, tp),
                device_id_type=MESH,
            ).start()

        each_partner(ep, 1, first, last, send, far_first)

    disp_send[...] = pick_quarter(tp)
    for group in range(GROUPS):
        dispatch(group * GROUP, (group + 1) * GROUP, disp_send, tp, disp_sems.at[group], False)
    rows[tp, 0] = disp_send[ep]
    disp_opposite[...] = pick_quarter(opposite)

    neighbours = (1, NTP - 1)
    others = (2, 1, NTP - 1)

    def own_bytes(group):
        return bytes_of(
            rows.at[0, pl.ds(0, GROUP - (group == 0))], disp_sems.at[group]
        )

    def spread_bytes(group):
        return bytes_of(rows.at[pl.ds(0, 2), pl.ds(group * GROUP, GROUP)], row_sems.at[group])

    for group in range(GROUPS):
        own_bytes(group).wait_recv()
        block = pl.ds(group * GROUP, GROUP)
        for d in neighbours:
            pltpu.make_async_remote_copy(
                src_ref=rows.at[tp, block],
                dst_ref=rows.at[tp, block],
                send_sem=row_sems.at[group, 0],
                recv_sem=row_sems.at[group, 1],
                device_id=(ep, (tp + d) % NTP),
                device_id_type=MESH,
            ).start()
        if group == 0:
            dispatch(0, NEP, disp_opposite, opposite, disp_sems.at[GROUPS], True)
            rows[opposite, 0] = disp_opposite[ep]

    for load in loads[6:]:
        load.wait()
    height = NEP * QMSG
    quarters = []

    def absorb(i, q):
        stage[i * height : (i + 1) * height, :] = rows[q].astype(F32).reshape(height, LANES)
        product = jnp.zeros((SLOTS, 2 * HIDDEN), F32)
        for j in range(0, QCHUNKS, 2):
            wide_rows = jnp.concatenate(
                [
                    jnp.concatenate(
                        [
                            stage[
                                pl.ds(
                                    i * height + group * GROUP * QMSG + (j + h) * CAP + c,
                                    GROUP,
                                    stride=QMSG,
                                ),
                                :,
                            ]
                            for group in range(GROUPS)
                            for c in range(CAP)
                        ],
                        axis=0,
                    )
                    for h in range(2)
                ],
                axis=1,
            ).astype(BF16)
            product = product + jnp.dot(
                wide_rows, gu_buf[q, j * LANES : (j + 2) * LANES, :], preferred_element_type=F32
            )
        quarters.append(product)

    opposite_bytes = bytes_of(rows.at[0, pl.ds(0, NEP - 1)], disp_sems.at[GROUPS])
    absorb(0, tp)
    opposite_bytes.wait_recv()
    absorb(1, opposite)
    for group in range(GROUPS):
        spread_bytes(group).wait_recv()
    absorb(2, (tp + 1) % NTP)
    absorb(3, (tp + 3) % NTP)
    gate_up = (quarters[0] + quarters[1]) + (quarters[2] + quarters[3])
    gate_part, up_part = gate_up[:, :HIDDEN], gate_up[:, HIDDEN:]
    hidden = (gate_part / (1.0 + jnp.exp(-gate_part)) * up_part).astype(BF16)

    def partial(q):
        return jnp.dot(hidden, down_buf[q], preferred_element_type=F32)

    def send_part(group, i):
        pltpu.make_async_remote_copy(
            src_ref=part_send.at[group, i],
            dst_ref=part_recv.at[group, i],
            send_sem=part_sems.at[group, 0],
            recv_sem=part_sems.at[group, 1],
            device_id=(ep, (tp + others[i]) % NTP),
            device_id_type=MESH,
        ).start()

    for i in range(NTP - 1):
        product = partial((tp + others[i]) % NTP).astype(BF16)
        for group in range(GROUPS):
            part_send[group, i] = product[group * GROUP * CAP : (group + 1) * GROUP * CAP]
        send_part(GROUPS - 1, i)
    for group in range(GROUPS - 2, -1, -1):
        for i in range(NTP - 1):
            send_part(group, i)

    def as_messages(product, group):
        for j in range(QCHUNKS):
            for c in range(CAP):
                ret_stage[pl.ds(group * GROUP * QMSG + j * CAP + c, GROUP, stride=QMSG), :] = (
                    product[c * GROUP : (c + 1) * GROUP, j * LANES : (j + 1) * LANES]
                )
        block = ret_stage[group * GROUP * QMSG : (group + 1) * GROUP * QMSG, :]
        return block.reshape(GROUP, QMSG, LANES).astype(BF16)

    def return_to(source, target, sems, lane_of_tp):
        def send(k, to):
            pltpu.make_async_remote_copy(
                src_ref=source.at[k],
                dst_ref=target.at[ep],
                send_sem=sems.at[0],
                recv_sem=sems.at[1],
                device_id=(to, lane_of_tp),
                device_id_type=MESH,
            ).start()

        return send

    own = partial(tp)
    send_own = return_to(ret_send, ret_recv, ret_sems, tp)
    for group in range(GROUPS - 1, -1, -1):
        bytes_of(part_recv.at[group], part_sems.at[group]).wait_recv()
        total = own[group * GROUP * CAP : (group + 1) * GROUP * CAP]
        for i in range(NTP - 1):
            total = total + part_recv[group, i].astype(F32)
        ret_send[group * GROUP : (group + 1) * GROUP] = as_messages(total, group)
        each_partner(ep, -1, group * GROUP, (group + 1) * GROUP, send_own, True)
    ret_recv[ep] = ret_send[0]

    bytes_of(heads.at[pl.ds(0, NTP - 1)], head_sems).wait_send()
    for group in range(GROUPS):
        own_bytes(group).wait_send()
        spread_bytes(group).wait_send()
        bytes_of(part_recv.at[group], part_sems.at[group]).wait_send()
    opposite_bytes.wait_send()
    from_own = bytes_of(ret_recv.at[pl.ds(0, NEP - 1)], ret_sems)
    from_own.wait_recv()
    returned = ret_recv[...].astype(F32).reshape(NEP * QMSG, LANES).astype(BF16)
    combined = jnp.dot(weigh_high, returned, preferred_element_type=F32) + jnp.dot(
        weigh_low, returned, preferred_element_type=F32
    )
    for j in range(QCHUNKS):
        output[:, j * LANES : (j + 1) * LANES] = (
            res_buf[tp, :, j * LANES : (j + 1) * LANES] + combined[j * ROWS : (j + 1) * ROWS]
        ).astype(BF16)
    from_own.wait_send()


def update_kernel(
    admitted_in,
    values_in,
    keep_in,
    memory,
    output_in,
    norm_in,
    stab_in,
    memory_next,
    output,
    norm_next,
    stabilizer_next,
    admitted,
    values,
    keep,
    mem_buf,
    output_buf,
    norm_buf,
    stab_buf,
    load_sem,
    store_sem,
):
    loads = [
        pltpu.make_async_copy(source, target, load_sem.at[i])
        for i, (source, target) in enumerate(
            (
                (admitted_in, admitted),
                (values_in, values),
                (keep_in, keep),
                (output_in, output_buf),
                (norm_in, norm_buf),
                (stab_in, stab_buf),
            )
        )
    ]
    blocks = [
        pltpu.make_async_copy(memory.at[s, 0], mem_buf.at[s], load_sem.at[6 + s])
        for s in range(ROWS)
    ]
    for load in loads + blocks:
        load.start()
    passed = [
        pltpu.make_async_copy(source, target, store_sem.at[ROWS + i])
        for i, (source, target) in enumerate(
            ((output_buf, output), (norm_buf, norm_next), (stab_buf, stabilizer_next))
        )
    ]
    for load in loads[:3]:
        load.wait()
    admitted_t = admitted[...].T
    for load, store in zip(loads[3:], passed, strict=True):
        load.wait()
        store.start()
    stores = []
    for s in range(ROWS):
        blocks[s].wait()
        mem_buf[s] = (
            keep[s : s + 1, 0:1] * mem_buf[s] + admitted_t[:, s : s + 1] * values[s : s + 1, :]
        )
        store = pltpu.make_async_copy(mem_buf.at[s], memory_next.at[s, 0], store_sem.at[s])
        store.start()
        stores.append(store)
    for store in passed + stores:
        store.wait()


def shards(
    tokens,
    w_query,
    w_key,
    w_value,
    w_outgate,
    w_igate,
    w_fgate,
    forget_bias,
    w_out,
    gain_mix,
    gain_moe,
    memory,
    normalizer,
    stabilizer,
    expert_gate,
    expert_up,
    expert_down,
    routes,
    route_weight,
):
    vmem = pl.BlockSpec(memory_space=pltpu.VMEM)
    smem = pl.BlockSpec(memory_space=pltpu.SMEM)
    hbm = pl.BlockSpec(memory_space=pl.ANY)
    smalls = (
        tokens,
        gain_mix.reshape(1, WIDTH),
        gain_moe.reshape(1, WIDTH),
        w_igate.reshape(1, WIDTH),
        w_fgate.reshape(1, WIDTH),
        normalizer,
        stabilizer.reshape(1, ROWS),
        routes.T,
        route_weight.T,
    )
    norm_shape = jax.ShapeDtypeStruct(normalizer.shape, F32)
    output_shape = jax.ShapeDtypeStruct((ROWS, QUARTER), BF16)
    stab_shape = jax.ShapeDtypeStruct((1, ROWS), F32)
    row_shape = jax.ShapeDtypeStruct((ROWS, HEAD), F32)
    keep_shape = jax.ShapeDtypeStruct((ROWS, LANES), F32)
    message = (QMSG, LANES)
    output, admitted, values, keep, norm_next, stab = pl.pallas_call(
        kernel,
        out_shape=(output_shape, row_shape, row_shape, keep_shape, norm_shape, stab_shape),
        in_specs=[hbm] * 18 + [smem],
        out_specs=(vmem,) * 6,
        scratch_shapes=[pltpu.VMEM(x.shape, x.dtype) for x in smalls]
        + [
            pltpu.VMEM((4, WIDTH, HEAD), BF16),
            pltpu.VMEM((ROWS, HEAD, HEAD), F32),
            pltpu.VMEM((HEAD, WIDTH), BF16),
            pltpu.VMEM((NTP, QUARTER, 2 * HIDDEN), BF16),
            pltpu.VMEM((NTP, HIDDEN, QUARTER), BF16),
            pltpu.VMEM((ROWS, HEAD), F32),
            pltpu.VMEM((NTP, ROWS, QUARTER), F32),
            pltpu.VMEM((NTP, ROWS, QUARTER), F32),
            pltpu.VMEM((NTP, ROWS, WIDTH), BF16),
            pltpu.VMEM((NTP * NEP * QMSG, LANES), F32),
            pltpu.VMEM((NEP, *message), BF16),
            pltpu.VMEM((NEP, *message), BF16),
            pltpu.VMEM((NTP, NEP, *message), BF16),
            pltpu.VMEM((GROUPS, NTP - 1, GROUP * CAP, QUARTER), BF16),
            pltpu.VMEM((GROUPS, NTP - 1, GROUP * CAP, QUARTER), BF16),
            pltpu.VMEM((NEP * QMSG, LANES), F32),
            pltpu.VMEM((NEP, *message), BF16),
            pltpu.VMEM((NEP, *message), BF16),
            pltpu.SemaphoreType.DMA((9,)),
            pltpu.SemaphoreType.DMA((12,)),
            pltpu.SemaphoreType.DMA((2,)),
            pltpu.SemaphoreType.DMA((GROUPS + 1, 2)),
            pltpu.SemaphoreType.DMA((GROUPS, 2)),
            pltpu.SemaphoreType.DMA((GROUPS, 2)),
            pltpu.SemaphoreType.DMA((2,)),
        ],
        compiler_params=pltpu.CompilerParams(
            collective_id=0, has_side_effects=True, vmem_limit_bytes=60 * 1024 * 1024
        ),
        name="layer",
    )(
        *smalls,
        w_key,
        w_value,
        w_query,
        w_outgate,
        memory,
        w_out,
        expert_gate.reshape(NTP, QUARTER, HIDDEN),
        expert_up.reshape(NTP, QUARTER, HIDDEN),
        expert_down,
        forget_bias,
    )
    memory_next, output, norm_next, stab = pl.pallas_call(
        update_kernel,
        out_shape=(
            jax.ShapeDtypeStruct(memory.shape, F32),
            output_shape,
            norm_shape,
            stab_shape,
        ),
        in_specs=[hbm] * 7,
        out_specs=(hbm,) * 4,
        scratch_shapes=[
            pltpu.VMEM((ROWS, HEAD), F32),
            pltpu.VMEM((ROWS, HEAD), F32),
            pltpu.VMEM((ROWS, LANES), F32),
            pltpu.VMEM((ROWS, HEAD, HEAD), F32),
            pltpu.VMEM(output_shape.shape, BF16),
            pltpu.VMEM(norm_shape.shape, F32),
            pltpu.VMEM(stab_shape.shape, F32),
            pltpu.SemaphoreType.DMA((6 + ROWS,)),
            pltpu.SemaphoreType.DMA((ROWS + 3,)),
        ],
        compiler_params=pltpu.CompilerParams(vmem_limit_bytes=60 * 1024 * 1024),
        name="update",
    )(admitted, values, keep, memory, output, norm_next, stab)
    return output, memory_next, norm_next, stab.reshape(ROWS, 1)


def solution(mesh):
    return jax.shard_map(
        shards,
        mesh=mesh,
        in_specs=(
            P("ep", None),
            P(None, "tp"),
            P(None, "tp"),
            P(None, "tp"),
            P(None, "tp"),
            P(None, "tp"),
            P(None, "tp"),
            P("tp"),
            P("tp", None),
            P(),
            P(),
            P("ep", "tp", None, None),
            P("ep", "tp", None),
            P("ep", "tp"),
            P("ep", None, "tp"),
            P("ep", None, "tp"),
            P("ep", "tp", None),
            P("ep", None),
            P("ep", None),
        ),
        out_specs=(P("ep", "tp"), P("ep", "tp", None, None), P("ep", "tp", None), P("ep", "tp")),
        check_vma=False,
    )
```

```python
import functools

import jax
import jax.numpy as jnp
from jax import lax
from jax.experimental import pallas as pl
from jax.experimental.pallas import tpu as pltpu
from jax.sharding import PartitionSpec as P

F32 = jnp.float32
BF16 = jnp.bfloat16
MESH = pl.DeviceIdType.MESH

ROWS = 8
WIDTH = 2048
HEAD = 256
HIDDEN = 128
TOP = 4
NEP = 64
NTP = 4
CAP = 2
SLOTS = NEP * CAP
LANES = 128
QUARTER = WIDTH // NTP
QCHUNKS = QUARTER // LANES
QMSG = QCHUNKS * CAP
GROUPS = 4
GROUP = NEP // GROUPS


def layer_norm(values, gain):
    mean = jnp.mean(values, -1, keepdims=True)
    centered = values - mean
    variance = jnp.mean(centered * centered, -1, keepdims=True)
    return centered * lax.rsqrt(variance + 1e-05) * gain


def iota(shape, dim):
    return lax.broadcasted_iota(jnp.int32, shape, dim)


def column(row, size):
    eye = iota((size, size), 0) == iota((size, size), 1)
    return jnp.sum(jnp.where(eye, row, 0.0), axis=1, keepdims=True)


def ring_step(k):
    return (k // 2) * (1 - 2 * (k % 2)) - k % 2


def each_partner(ep, sign, first, last, act, far_first=False):
    z, y, c = ep // 8, (ep // 2) % 4, ep % 2
    columns = [
        ((y + sign * ring_step(m) + 4) % 4) * 2 + (c + sign * dc + 2) % 2
        for m in range(4)
        for dc in (0, 1)
    ]
    low, high = max(first // 8, 1), last // 8

    def plane(a, start):
        base = ((z + sign * ring_step(a) + 8) % 8) * 8
        order = range(7, start - 1, -1) if far_first else range(start, 8)
        for b in order:
            act(a * 8 + b, base + columns[b])

    def whole(i, carry):
        plane(low + high - 1 - i if far_first else i, 0)
        return carry

    if first == 0 and not far_first:
        plane(0, 1)
    lax.fori_loop(low, high, whole, 0)
    if first == 0 and far_first:
        plane(0, 1)


def kernel(
    tokens_in,
    gain_mix_in,
    gain_moe_in,
    w_igate_in,
    w_fgate_in,
    normalizer_in,
    stabilizer_in,
    routes_in,
    route_weight_in,
    w_key,
    w_value,
    w_query,
    w_outgate,
    memory,
    w_out,
    expert_gate,
    expert_up,
    expert_down,
    forget_bias,
    output_hbm,
    admitted_hbm,
    values_hbm,
    keep_hbm,
    norm_hbm,
    stabilizer_hbm,
    output,
    admitted_out,
    values_out,
    keep_out,
    norm_next,
    stabilizer_next,
    tokens,
    gain_mix,
    gain_moe,
    w_igate,
    w_fgate,
    normalizer,
    stabilizer,
    routes,
    route_weight,
    w_buf,
    mem_buf,
    out_buf,
    gu_buf,
    down_buf,
    num_buf,
    res_buf,
    in_buf,
    heads,
    stage,
    disp_send,
    disp_opposite,
    rows,
    part_send,
    part_recv,
    ret_stage,
    ret_send,
    ret_recv,
    opp_send,
    opp_recv,
    cross_send,
    cross_recv,
    small_sem,
    load_sem,
    head_sems,
    disp_sems,
    row_sems,
    part_sems,
    ret_sems,
    out_sem,
):
    ep = lax.axis_index("ep")
    tp = lax.axis_index("tp")

    smalls = [
        pltpu.make_async_copy(source, target, small_sem.at[i])
        for i, (source, target) in enumerate(
            (
                (tokens_in, tokens),
                (gain_mix_in, gain_mix),
                (w_igate_in, w_igate),
                (w_fgate_in, w_fgate),
                (stabilizer_in, stabilizer),
                (normalizer_in, normalizer),
                (gain_moe_in, gain_moe),
                (routes_in, routes),
                (route_weight_in, route_weight),
            )
        )
    ]
    loads = [
        pltpu.make_async_copy(w, w_buf.at[i], load_sem.at[i])
        for i, w in enumerate((w_key, w_value, w_query, w_outgate))
    ]
    loads.append(pltpu.make_async_copy(memory.at[:, 0], mem_buf, load_sem.at[4]))
    loads.append(pltpu.make_async_copy(w_out, out_buf, load_sem.at[5]))
    loads.append(
        pltpu.make_async_copy(expert_gate, gu_buf.at[:, :, pl.ds(0, HIDDEN)], load_sem.at[6])
    )
    loads.append(
        pltpu.make_async_copy(
            expert_up, gu_buf.at[:, :, pl.ds(HIDDEN, HIDDEN)], load_sem.at[7]
        )
    )
    for q in range(NTP):
        loads.append(
            pltpu.make_async_copy(
                expert_down.at[0, :, pl.ds(q * QUARTER, QUARTER)],
                down_buf.at[q],
                load_sem.at[8 + q],
            )
        )
    for small in smalls:
        small.start()

    barrier = pltpu.get_barrier_semaphore()
    opposite = (tp + 2) % NTP

    def greet(k, index):
        pl.semaphore_signal(barrier, inc=1, device_id=(index, tp), device_id_type=MESH)

    each_partner(ep, 1, NEP // 2, NEP, greet, far_first=True)
    for load in loads[:3]:
        load.start()
    each_partner(ep, 1, 0, NEP // 2, greet, far_first=True)
    for d in range(1, NTP):
        pl.semaphore_signal(
            barrier, inc=1, device_id=(ep, (tp + d) % NTP), device_id_type=MESH
        )

    for small in smalls[:6]:
        small.wait()
    token_rows = tokens[...].astype(F32)
    normed = layer_norm(token_rows, gain_mix[...]).astype(BF16)
    wide = normed.astype(F32)
    gate_in = jnp.sum(wide * w_igate[...].astype(F32), axis=1, keepdims=True)
    gate_forget = jnp.sum(wide * w_fgate[...].astype(F32), axis=1, keepdims=True)
    shifted = gate_forget + forget_bias[0]
    log_forget = jnp.minimum(shifted, 0.0) - jnp.log1p(jnp.exp(-jnp.abs(shifted)))
    carried = log_forget + column(stabilizer[...], ROWS)
    stab = jnp.maximum(carried, gate_in)
    keep = jnp.exp(carried - stab)
    admit = jnp.exp(gate_in - stab)
    eye = iota((ROWS, ROWS), 0) == iota((ROWS, ROWS), 1)
    stabilizer_next[...] = jnp.sum(jnp.where(eye, stab, 0.0), axis=0, keepdims=True)

    def project(i):
        loads[i].wait()
        product = jnp.dot(normed, w_buf[i], preferred_element_type=F32)
        return product.astype(BF16).astype(F32)

    loads[4].start()
    keys = project(0) * (1.0 / 16.0)
    loads[3].start()
    loads[5].start()
    values = project(1)
    queries = project(2)
    admitted = admit * keys
    new_norm = keep * normalizer[:, 0, :] + admitted
    norm_next[:, 0, :] = new_norm
    admitted_out[...] = admitted
    values_out[...] = values
    keep_out[...] = jnp.broadcast_to(keep, (ROWS, LANES))
    denominator = jnp.sum(queries * new_norm, axis=1, keepdims=True)
    admitted_t = admitted.T
    queries_t = queries.T
    loads[4].wait()
    step = 64
    for s in range(ROWS):
        total = jnp.zeros((8, HEAD), F32)
        rate = keep[s : s + 1, :]
        value_row = values[s : s + 1, :]
        for r in range(0, HEAD, step):
            block = (
                rate * mem_buf[s, r : r + step, :]
                + admitted_t[r : r + step, s : s + 1] * value_row
            )
            weighed = queries_t[r : r + step, s : s + 1] * block
            total = total + jnp.sum(weighed.reshape(step // 8, 8, HEAD), axis=0)
        num_buf[s : s + 1, :] = jnp.sum(total, axis=0, keepdims=True)
    out_gate = project(3)
    readout = num_buf[...] / jnp.maximum(jnp.abs(denominator), jnp.exp(-stab))
    mixed = (readout / (1.0 + jnp.exp(-out_gate))).astype(BF16)
    loads[5].wait()
    heads[tp] = jnp.dot(mixed, out_buf[...], preferred_element_type=F32).astype(BF16)

    pl.semaphore_wait(barrier, NEP - 1 + NTP - 1)
    for d in (2, 1, 3):
        pltpu.make_async_remote_copy(
            src_ref=heads.at[tp],
            dst_ref=heads.at[tp],
            send_sem=head_sems.at[0],
            recv_sem=head_sems.at[1],
            device_id=(ep, (tp + d) % NTP),
            device_id_type=MESH,
        ).start()

    for load in loads[6:]:
        load.start()

    stores = [
        pltpu.make_async_copy(source, target, out_sem.at[i])
        for i, (source, target) in enumerate(
            (
                (output, output_hbm),
                (admitted_out, admitted_hbm),
                (values_out, values_hbm),
                (keep_out, keep_hbm),
                (norm_next, norm_hbm),
                (stabilizer_next, stabilizer_hbm),
            )
        )
    ]
    for store in stores[1:]:
        store.start()

    for small in smalls[6:]:
        small.wait()
    route_rows = routes[...].astype(F32)
    earlier = iota((ROWS, ROWS), 0) < iota((ROWS, ROWS), 1)
    targets = []
    for choice in range(TOP):
        mine = route_rows[choice : choice + 1, :]
        same = jnp.zeros((ROWS, ROWS), F32)
        for other in range(TOP):
            theirs = column(route_rows[other : other + 1, :], ROWS)
            same = same + jnp.where((theirs == mine) & earlier, 1.0, 0.0)
        targets.append(mine * CAP + jnp.sum(same, axis=0, keepdims=True))
    tall = QCHUNKS * ROWS
    copies = iota((tall, ROWS), 0) % ROWS == iota((tall, ROWS), 1)
    tall_chunk = (iota((tall, 1), 0) // ROWS).astype(F32)
    lane = iota((1, NEP * QMSG), 1)
    lane_key = (((lane // QMSG) * CAP + lane % CAP) * QCHUNKS + (lane % QMSG) // CAP).astype(F32)
    weigh = jnp.zeros((tall, NEP * QMSG), F32)
    filled = jnp.zeros((tall, NEP * QMSG), F32)
    for choice in range(TOP):
        tall_key = (
            jnp.sum(jnp.where(copies, targets[choice], 0.0), axis=1, keepdims=True) * QCHUNKS
            + tall_chunk
        )
        weight = jnp.sum(
            jnp.where(copies, route_weight[choice : choice + 1, :], 0.0), axis=1, keepdims=True
        )
        hit = tall_key == lane_key
        weigh = weigh + jnp.where(hit, weight, 0.0)
        filled = filled + jnp.where(hit, 1.0, 0.0)
    weigh_high = weigh.astype(BF16)
    weigh_low = (weigh - weigh_high.astype(F32)).astype(BF16)
    pick = filled.T.astype(BF16)

    def bytes_of(view, sems):
        return pltpu.make_async_remote_copy(
            src_ref=view,
            dst_ref=view,
            send_sem=sems.at[0],
            recv_sem=sems.at[1],
            device_id=(ep, tp),
            device_id_type=MESH,
        )

    bytes_of(heads.at[pl.ds(0, NTP - 1)], head_sems).wait_recv()
    summed = heads[0].astype(F32)
    for h in range(1, NTP):
        summed = summed + heads[h].astype(F32)
    residual = token_rows + summed
    expert_in = layer_norm(residual, gain_moe[...])
    for q in range(NTP):
        res_buf[q] = residual[:, q * QUARTER : (q + 1) * QUARTER]
        in_buf[q] = expert_in[:, q * QUARTER : (q + 1) * QUARTER]

    def pick_quarter(q):
        stacked = jnp.concatenate(
            [in_buf[q, :, j * LANES : (j + 1) * LANES] for j in range(QCHUNKS)], axis=0
        ).astype(BF16)
        picked = jnp.dot(pick, stacked, preferred_element_type=F32).astype(BF16)
        return picked.reshape(NEP, QMSG, LANES)

    def dispatch(first, last, source, q, sems, far_first):
        def send(k, to):
            pltpu.make_async_remote_copy(
                src_ref=source.at[to],
                dst_ref=rows.at[q, k],
                send_sem=sems.at[0],
                recv_sem=sems.at[1],
                device_id=(to, tp),
                device_id_type=MESH,
            ).start()

        each_partner(ep, 1, first, last, send, far_first)

    disp_send[...] = pick_quarter(tp)
    for group in range(GROUPS):
        dispatch(group * GROUP, (group + 1) * GROUP, disp_send, tp, disp_sems.at[group], False)
    rows[tp, 0] = disp_send[ep]
    disp_opposite[...] = pick_quarter(opposite)

    neighbours = (1, NTP - 1)

    def own_bytes(group):
        return bytes_of(
            rows.at[0, pl.ds(0, GROUP - (group == 0))], disp_sems.at[group]
        )

    def spread_bytes(group):
        return bytes_of(rows.at[pl.ds(0, 2), pl.ds(group * GROUP, GROUP)], row_sems.at[group])

    for group in range(GROUPS):
        own_bytes(group).wait_recv()
        block = pl.ds(group * GROUP, GROUP)
        for d in neighbours:
            pltpu.make_async_remote_copy(
                src_ref=rows.at[tp, block],
                dst_ref=rows.at[tp, block],
                send_sem=row_sems.at[group, 0],
                recv_sem=row_sems.at[group, 1],
                device_id=(ep, (tp + d) % NTP),
                device_id_type=MESH,
            ).start()
        if group == 0:
            dispatch(0, NEP, disp_opposite, opposite, disp_sems.at[GROUPS], True)
            rows[opposite, 0] = disp_opposite[ep]

    for load in loads[6:]:
        load.wait()
    height = NEP * QMSG
    quarters = []

    def absorb(i, q):
        stage[i * height : (i + 1) * height, :] = rows[q].astype(F32).reshape(height, LANES)
        product = jnp.zeros((SLOTS, 2 * HIDDEN), F32)
        for j in range(0, QCHUNKS, 2):
            wide_rows = jnp.concatenate(
                [
                    jnp.concatenate(
                        [
                            stage[
                                pl.ds(
                                    i * height + group * GROUP * QMSG + (j + h) * CAP + c,
                                    GROUP,
                                    stride=QMSG,
                                ),
                                :,
                            ]
                            for group in range(GROUPS)
                            for c in range(CAP)
                        ],
                        axis=0,
                    )
                    for h in range(2)
                ],
                axis=1,
            ).astype(BF16)
            product = product + jnp.dot(
                wide_rows, gu_buf[q, j * LANES : (j + 2) * LANES, :], preferred_element_type=F32
            )
        quarters.append(product)

    opposite_bytes = bytes_of(rows.at[0, pl.ds(0, NEP - 1)], disp_sems.at[GROUPS])
    absorb(0, tp)
    opposite_bytes.wait_recv()
    absorb(1, opposite)
    for group in range(GROUPS):
        spread_bytes(group).wait_recv()
    absorb(2, (tp + 1) % NTP)
    absorb(3, (tp + 3) % NTP)
    gate_up = (quarters[0] + quarters[1]) + (quarters[2] + quarters[3])
    gate_part, up_part = gate_up[:, :HIDDEN], gate_up[:, HIDDEN:]
    hidden = (gate_part / (1.0 + jnp.exp(-gate_part)) * up_part).astype(BF16)

    def partial(q):
        return jnp.dot(hidden, down_buf[q], preferred_element_type=F32)

    def send_part(group, i):
        pltpu.make_async_remote_copy(
            src_ref=part_send.at[group, i],
            dst_ref=part_recv.at[group, i],
            send_sem=part_sems.at[group, 0],
            recv_sem=part_sems.at[group, 1],
            device_id=(ep, (tp + neighbours[i]) % NTP),
            device_id_type=MESH,
        ).start()

    for i in range(2):
        product = partial((tp + neighbours[i]) % NTP).astype(BF16)
        for group in range(GROUPS):
            part_send[group, i] = product[group * GROUP * CAP : (group + 1) * GROUP * CAP]
        send_part(GROUPS - 1, i)
    for group in range(GROUPS - 2, -1, -1):
        for i in range(2):
            send_part(group, i)

    def as_messages(product, group):
        for j in range(QCHUNKS):
            for c in range(CAP):
                ret_stage[pl.ds(group * GROUP * QMSG + j * CAP + c, GROUP, stride=QMSG), :] = (
                    product[c * GROUP : (c + 1) * GROUP, j * LANES : (j + 1) * LANES]
                )
        block = ret_stage[group * GROUP * QMSG : (group + 1) * GROUP * QMSG, :]
        return block.reshape(GROUP, QMSG, LANES).astype(BF16)

    def return_to(source, target, sems, lane_of_tp):
        def send(k, to):
            pltpu.make_async_remote_copy(
                src_ref=source.at[k],
                dst_ref=target.at[ep],
                send_sem=sems.at[0],
                recv_sem=sems.at[1],
                device_id=(to, lane_of_tp),
                device_id_type=MESH,
            ).start()

        return send

    product = partial(opposite)
    for group in range(GROUPS):
        opp_send[group * GROUP : (group + 1) * GROUP] = as_messages(
            product[group * GROUP * CAP : (group + 1) * GROUP * CAP], group
        )
    each_partner(ep, -1, 0, NEP, return_to(opp_send, opp_recv, ret_sems.at[1], tp), True)
    opp_recv[ep] = opp_send[0]

    own = partial(tp)
    send_own = return_to(ret_send, ret_recv, ret_sems.at[0], tp)
    for group in range(GROUPS - 1, -1, -1):
        bytes_of(part_recv.at[group], part_sems.at[group]).wait_recv()
        total = own[group * GROUP * CAP : (group + 1) * GROUP * CAP]
        for i in range(2):
            total = total + part_recv[group, i].astype(F32)
        ret_send[group * GROUP : (group + 1) * GROUP] = as_messages(total, group)
        each_partner(ep, -1, group * GROUP, (group + 1) * GROUP, send_own, True)
    ret_recv[ep] = ret_send[0]


    def weighted(buffer):
        returned = buffer[...].astype(F32).reshape(NEP * QMSG, LANES).astype(BF16)
        return jnp.dot(weigh_high, returned, preferred_element_type=F32) + jnp.dot(
            weigh_low, returned, preferred_element_type=F32
        )

    back = [
        bytes_of(buffer.at[pl.ds(0, NEP - 1)], ret_sems.at[i])
        for i, buffer in enumerate((ret_recv, opp_recv))
    ]
    back[1].wait_recv()
    cross_send[...] = weighted(opp_recv)
    cross = pltpu.make_async_remote_copy(
        src_ref=cross_send,
        dst_ref=cross_recv,
        send_sem=ret_sems.at[2, 0],
        recv_sem=ret_sems.at[2, 1],
        device_id=(ep, opposite),
        device_id_type=MESH,
    )
    cross.start()
    bytes_of(heads.at[pl.ds(0, NTP - 1)], head_sems).wait_send()
    for group in range(GROUPS):
        own_bytes(group).wait_send()
        spread_bytes(group).wait_send()
        bytes_of(part_recv.at[group], part_sems.at[group]).wait_send()
    opposite_bytes.wait_send()
    back[0].wait_recv()
    combined = weighted(ret_recv)
    cross.wait_recv()
    combined = combined + cross_recv[...]
    for j in range(QCHUNKS):
        output[:, j * LANES : (j + 1) * LANES] = (
            res_buf[tp, :, j * LANES : (j + 1) * LANES] + combined[j * ROWS : (j + 1) * ROWS]
        ).astype(BF16)
    stores[0].start()
    cross.wait_send()
    for messages in back:
        messages.wait_send()
    for store in stores:
        store.wait()


def update_kernel(
    admitted_in,
    values_in,
    keep_in,
    memory,
    output_in,
    norm_in,
    stab_in,
    memory_next,
    output,
    norm_next,
    stabilizer_next,
    admitted,
    values,
    keep,
    mem_buf,
    output_buf,
    norm_buf,
    stab_buf,
    load_sem,
    store_sem,
):
    loads = [
        pltpu.make_async_copy(source, target, load_sem.at[i])
        for i, (source, target) in enumerate(
            (
                (admitted_in, admitted),
                (values_in, values),
                (keep_in, keep),
                (output_in, output_buf),
                (norm_in, norm_buf),
                (stab_in, stab_buf),
            )
        )
    ]
    blocks = [
        pltpu.make_async_copy(memory.at[s, 0], mem_buf.at[s], load_sem.at[6 + s])
        for s in range(ROWS)
    ]
    for load in loads + blocks:
        load.start()
    passed = [
        pltpu.make_async_copy(source, target, store_sem.at[ROWS + i])
        for i, (source, target) in enumerate(
            ((output_buf, output), (norm_buf, norm_next), (stab_buf, stabilizer_next))
        )
    ]
    for load in loads[:3]:
        load.wait()
    admitted_t = admitted[...].T
    for load, store in zip(loads[3:], passed, strict=True):
        load.wait()
        store.start()
    stores = []
    for s in range(ROWS):
        blocks[s].wait()
        mem_buf[s] = (
            keep[s : s + 1, 0:1] * mem_buf[s] + admitted_t[:, s : s + 1] * values[s : s + 1, :]
        )
        store = pltpu.make_async_copy(mem_buf.at[s], memory_next.at[s, 0], store_sem.at[s])
        store.start()
        stores.append(store)
    for store in passed + stores:
        store.wait()


def shards(
    tokens,
    w_query,
    w_key,
    w_value,
    w_outgate,
    w_igate,
    w_fgate,
    forget_bias,
    w_out,
    gain_mix,
    gain_moe,
    memory,
    normalizer,
    stabilizer,
    expert_gate,
    expert_up,
    expert_down,
    routes,
    route_weight,
):
    vmem = pl.BlockSpec(memory_space=pltpu.VMEM)
    smem = pl.BlockSpec(memory_space=pltpu.SMEM)
    hbm = pl.BlockSpec(memory_space=pl.ANY)
    smalls = (
        tokens,
        gain_mix.reshape(1, WIDTH),
        gain_moe.reshape(1, WIDTH),
        w_igate.reshape(1, WIDTH),
        w_fgate.reshape(1, WIDTH),
        normalizer,
        stabilizer.reshape(1, ROWS),
        routes.T,
        route_weight.T,
    )
    norm_shape = jax.ShapeDtypeStruct(normalizer.shape, F32)
    output_shape = jax.ShapeDtypeStruct((ROWS, QUARTER), BF16)
    stab_shape = jax.ShapeDtypeStruct((1, ROWS), F32)
    row_shape = jax.ShapeDtypeStruct((ROWS, HEAD), F32)
    keep_shape = jax.ShapeDtypeStruct((ROWS, LANES), F32)
    message = (QMSG, LANES)
    results = (output_shape, row_shape, row_shape, keep_shape, norm_shape, stab_shape)
    output, admitted, values, keep, norm_next, stab = pl.pallas_call(
        kernel,
        out_shape=results,
        in_specs=[hbm] * 18 + [smem],
        out_specs=(hbm,) * 6,
        scratch_shapes=[pltpu.VMEM(x.shape, x.dtype) for x in (*results, *smalls)]
        + [
            pltpu.VMEM((4, WIDTH, HEAD), BF16),
            pltpu.VMEM((ROWS, HEAD, HEAD), F32),
            pltpu.VMEM((HEAD, WIDTH), BF16),
            pltpu.VMEM((NTP, QUARTER, 2 * HIDDEN), BF16),
            pltpu.VMEM((NTP, HIDDEN, QUARTER), BF16),
            pltpu.VMEM((ROWS, HEAD), F32),
            pltpu.VMEM((NTP, ROWS, QUARTER), F32),
            pltpu.VMEM((NTP, ROWS, QUARTER), F32),
            pltpu.VMEM((NTP, ROWS, WIDTH), BF16),
            pltpu.VMEM((NTP * NEP * QMSG, LANES), F32),
            pltpu.VMEM((NEP, *message), BF16),
            pltpu.VMEM((NEP, *message), BF16),
            pltpu.VMEM((NTP, NEP, *message), BF16),
            pltpu.VMEM((GROUPS, 2, GROUP * CAP, QUARTER), BF16),
            pltpu.VMEM((GROUPS, 2, GROUP * CAP, QUARTER), BF16),
            pltpu.VMEM((NEP * QMSG, LANES), F32),
            pltpu.VMEM((NEP, *message), BF16),
            pltpu.VMEM((NEP, *message), BF16),
            pltpu.VMEM((NEP, *message), BF16),
            pltpu.VMEM((NEP, *message), BF16),
            pltpu.VMEM((QCHUNKS * ROWS, LANES), F32),
            pltpu.VMEM((QCHUNKS * ROWS, LANES), F32),
            pltpu.SemaphoreType.DMA((9,)),
            pltpu.SemaphoreType.DMA((12,)),
            pltpu.SemaphoreType.DMA((2,)),
            pltpu.SemaphoreType.DMA((GROUPS + 1, 2)),
            pltpu.SemaphoreType.DMA((GROUPS, 2)),
            pltpu.SemaphoreType.DMA((GROUPS, 2)),
            pltpu.SemaphoreType.DMA((3, 2)),
            pltpu.SemaphoreType.DMA((6,)),
        ],
        compiler_params=pltpu.CompilerParams(
            collective_id=0, has_side_effects=True, vmem_limit_bytes=60 * 1024 * 1024
        ),
        name="layer",
    )(
        *smalls,
        w_key,
        w_value,
        w_query,
        w_outgate,
        memory,
        w_out,
        expert_gate.reshape(NTP, QUARTER, HIDDEN),
        expert_up.reshape(NTP, QUARTER, HIDDEN),
        expert_down,
        forget_bias,
    )
    memory_next, output, norm_next, stab = pl.pallas_call(
        update_kernel,
        out_shape=(
            jax.ShapeDtypeStruct(memory.shape, F32),
            output_shape,
            norm_shape,
            stab_shape,
        ),
        in_specs=[hbm] * 7,
        out_specs=(hbm,) * 4,
        scratch_shapes=[
            pltpu.VMEM((ROWS, HEAD), F32),
            pltpu.VMEM((ROWS, HEAD), F32),
            pltpu.VMEM((ROWS, LANES), F32),
            pltpu.VMEM((ROWS, HEAD, HEAD), F32),
            pltpu.VMEM(output_shape.shape, BF16),
            pltpu.VMEM(norm_shape.shape, F32),
            pltpu.VMEM(stab_shape.shape, F32),
            pltpu.SemaphoreType.DMA((6 + ROWS,)),
            pltpu.SemaphoreType.DMA((ROWS + 3,)),
        ],
        compiler_params=pltpu.CompilerParams(vmem_limit_bytes=60 * 1024 * 1024),
        name="update",
    )(admitted, values, keep, memory, output, norm_next, stab)
    return output, memory_next, norm_next, stab.reshape(ROWS, 1)


def solution(mesh):
    return jax.shard_map(
        shards,
        mesh=mesh,
        in_specs=(
            P("ep", None),
            P(None, "tp"),
            P(None, "tp"),
            P(None, "tp"),
            P(None, "tp"),
            P(None, "tp"),
            P(None, "tp"),
            P("tp"),
            P("tp", None),
            P(),
            P(),
            P("ep", "tp", None, None),
            P("ep", "tp", None),
            P("ep", "tp"),
            P("ep", None, "tp"),
            P("ep", None, "tp"),
            P("ep", "tp", None),
            P("ep", None),
            P("ep", None),
        ),
        out_specs=(P("ep", "tp"), P("ep", "tp", None, None), P("ep", "tp", None), P("ep", "tp")),
        check_vma=False,
    )
```

```python
import functools

import jax
import jax.numpy as jnp
from jax import lax
from jax.experimental import pallas as pl
from jax.experimental.pallas import tpu as pltpu
from jax.sharding import PartitionSpec as P

F32 = jnp.float32
BF16 = jnp.bfloat16
MESH = pl.DeviceIdType.MESH

ROWS = 8
WIDTH = 2048
HEAD = 256
HIDDEN = 128
TOP = 4
NEP = 64
NTP = 4
CAP = 2
SLOTS = NEP * CAP
LANES = 128
QUARTER = WIDTH // NTP
QCHUNKS = QUARTER // LANES
QMSG = QCHUNKS * CAP
GROUPS = 4
GROUP = NEP // GROUPS


def layer_norm(values, gain):
    mean = jnp.mean(values, -1, keepdims=True)
    centered = values - mean
    variance = jnp.mean(centered * centered, -1, keepdims=True)
    return centered * lax.rsqrt(variance + 1e-05) * gain


def iota(shape, dim):
    return lax.broadcasted_iota(jnp.int32, shape, dim)


def column(row, size):
    eye = iota((size, size), 0) == iota((size, size), 1)
    return jnp.sum(jnp.where(eye, row, 0.0), axis=1, keepdims=True)


def ring_step(k):
    return (k // 2) * (1 - 2 * (k % 2)) - k % 2


def each_partner(ep, sign, first, last, act, far_first=False):
    z, y, c = ep // 8, (ep // 2) % 4, ep % 2
    columns = [
        ((y + sign * ring_step(m) + 4) % 4) * 2 + (c + sign * dc + 2) % 2
        for m in range(4)
        for dc in (0, 1)
    ]
    low, high = max(first // 8, 1), last // 8

    def plane(a, start):
        base = ((z + sign * ring_step(a) + 8) % 8) * 8
        order = range(7, start - 1, -1) if far_first else range(start, 8)
        for b in order:
            act(a * 8 + b, base + columns[b])

    def whole(i, carry):
        plane(low + high - 1 - i if far_first else i, 0)
        return carry

    if first == 0 and not far_first:
        plane(0, 1)
    lax.fori_loop(low, high, whole, 0)
    if first == 0 and far_first:
        plane(0, 1)


def kernel(
    tokens_in,
    gain_mix_in,
    gain_moe_in,
    w_igate_in,
    w_fgate_in,
    normalizer_in,
    stabilizer_in,
    routes_in,
    route_weight_in,
    w_key,
    w_value,
    w_query,
    w_outgate,
    memory,
    w_out,
    expert_gate,
    expert_up,
    expert_down,
    forget_bias,
    output_hbm,
    admitted_hbm,
    values_hbm,
    keep_hbm,
    norm_hbm,
    stabilizer_hbm,
    output,
    admitted_out,
    values_out,
    keep_out,
    norm_next,
    stabilizer_next,
    tokens,
    gain_mix,
    gain_moe,
    w_igate,
    w_fgate,
    normalizer,
    stabilizer,
    routes,
    route_weight,
    w_buf,
    mem_buf,
    out_buf,
    gu_buf,
    down_buf,
    num_buf,
    res_buf,
    in_buf,
    heads,
    stage,
    disp_send,
    disp_opposite,
    rows,
    part_send,
    part_recv,
    ret_stage,
    ret_send,
    ret_recv,
    opp_send,
    opp_recv,
    cross_send,
    cross_recv,
    small_sem,
    load_sem,
    head_sems,
    disp_sems,
    row_sems,
    part_sems,
    ret_sems,
    out_sem,
):
    ep = lax.axis_index("ep")
    tp = lax.axis_index("tp")

    smalls = [
        pltpu.make_async_copy(source, target, small_sem.at[i])
        for i, (source, target) in enumerate(
            (
                (tokens_in, tokens),
                (gain_mix_in, gain_mix),
                (w_igate_in, w_igate),
                (w_fgate_in, w_fgate),
                (stabilizer_in, stabilizer),
                (normalizer_in, normalizer),
                (gain_moe_in, gain_moe),
                (routes_in, routes),
                (route_weight_in, route_weight),
            )
        )
    ]
    loads = [
        pltpu.make_async_copy(w, w_buf.at[i], load_sem.at[i])
        for i, w in enumerate((w_key, w_value, w_query, w_outgate))
    ]
    loads.append(pltpu.make_async_copy(memory.at[:, 0], mem_buf, load_sem.at[4]))
    loads.append(pltpu.make_async_copy(w_out, out_buf, load_sem.at[5]))
    loads.append(
        pltpu.make_async_copy(expert_gate, gu_buf.at[:, :, pl.ds(0, HIDDEN)], load_sem.at[6])
    )
    loads.append(
        pltpu.make_async_copy(
            expert_up, gu_buf.at[:, :, pl.ds(HIDDEN, HIDDEN)], load_sem.at[7]
        )
    )
    for q in range(NTP):
        loads.append(
            pltpu.make_async_copy(
                expert_down.at[0, :, pl.ds(q * QUARTER, QUARTER)],
                down_buf.at[q],
                load_sem.at[8 + q],
            )
        )
    for small in smalls:
        small.start()

    barrier = pltpu.get_barrier_semaphore()
    opposite = (tp + 2) % NTP

    def greet(k, index):
        pl.semaphore_signal(barrier, inc=1, device_id=(index, tp), device_id_type=MESH)

    each_partner(ep, 1, NEP // 2, NEP, greet, far_first=True)
    for load in loads[:3]:
        load.start()
    each_partner(ep, 1, 0, NEP // 2, greet, far_first=True)
    for d in range(1, NTP):
        pl.semaphore_signal(
            barrier, inc=1, device_id=(ep, (tp + d) % NTP), device_id_type=MESH
        )

    for small in smalls[:6]:
        small.wait()
    token_rows = tokens[...].astype(F32)
    normed = layer_norm(token_rows, gain_mix[...]).astype(BF16)
    wide = normed.astype(F32)
    gate_in = jnp.sum(wide * w_igate[...].astype(F32), axis=1, keepdims=True)
    gate_forget = jnp.sum(wide * w_fgate[...].astype(F32), axis=1, keepdims=True)
    shifted = gate_forget + forget_bias[0]
    log_forget = jnp.minimum(shifted, 0.0) - jnp.log1p(jnp.exp(-jnp.abs(shifted)))
    carried = log_forget + column(stabilizer[...], ROWS)
    stab = jnp.maximum(carried, gate_in)
    keep = jnp.exp(carried - stab)
    admit = jnp.exp(gate_in - stab)
    eye = iota((ROWS, ROWS), 0) == iota((ROWS, ROWS), 1)
    stabilizer_next[...] = jnp.sum(jnp.where(eye, stab, 0.0), axis=0, keepdims=True)

    def project(i):
        loads[i].wait()
        product = jnp.dot(normed, w_buf[i], preferred_element_type=F32)
        return product.astype(BF16).astype(F32)

    loads[4].start()
    keys = project(0) * (1.0 / 16.0)
    loads[3].start()
    loads[5].start()
    values = project(1)
    queries = project(2)
    admitted = admit * keys
    new_norm = keep * normalizer[:, 0, :] + admitted
    norm_next[:, 0, :] = new_norm
    admitted_out[...] = admitted
    values_out[...] = values
    keep_out[...] = jnp.broadcast_to(keep, (ROWS, LANES))
    denominator = jnp.sum(queries * new_norm, axis=1, keepdims=True)
    admitted_t = admitted.T
    queries_t = queries.T
    loads[4].wait()
    step = 64
    for s in range(ROWS):
        total = jnp.zeros((8, HEAD), F32)
        rate = keep[s : s + 1, :]
        value_row = values[s : s + 1, :]
        for r in range(0, HEAD, step):
            block = (
                rate * mem_buf[s, r : r + step, :]
                + admitted_t[r : r + step, s : s + 1] * value_row
            )
            weighed = queries_t[r : r + step, s : s + 1] * block
            total = total + jnp.sum(weighed.reshape(step // 8, 8, HEAD), axis=0)
        num_buf[s : s + 1, :] = jnp.sum(total, axis=0, keepdims=True)
    out_gate = project(3)
    readout = num_buf[...] / jnp.maximum(jnp.abs(denominator), jnp.exp(-stab))
    mixed = (readout / (1.0 + jnp.exp(-out_gate))).astype(BF16)
    loads[5].wait()
    heads[tp] = jnp.dot(mixed, out_buf[...], preferred_element_type=F32).astype(BF16)

    pl.semaphore_wait(barrier, NEP - 1 + NTP - 1)
    for d in (2, 1, 3):
        pltpu.make_async_remote_copy(
            src_ref=heads.at[tp],
            dst_ref=heads.at[tp],
            send_sem=head_sems.at[0],
            recv_sem=head_sems.at[1],
            device_id=(ep, (tp + d) % NTP),
            device_id_type=MESH,
        ).start()

    for load in loads[6:]:
        load.start()

    stores = [
        pltpu.make_async_copy(source, target, out_sem.at[i])
        for i, (source, target) in enumerate(
            (
                (output, output_hbm),
                (admitted_out, admitted_hbm),
                (values_out, values_hbm),
                (keep_out, keep_hbm),
                (norm_next, norm_hbm),
                (stabilizer_next, stabilizer_hbm),
            )
        )
    ]
    for store in stores[1:]:
        store.start()

    for small in smalls[6:]:
        small.wait()
    route_rows = routes[...].astype(F32)
    earlier = iota((ROWS, ROWS), 0) < iota((ROWS, ROWS), 1)
    targets = []
    for choice in range(TOP):
        mine = route_rows[choice : choice + 1, :]
        same = jnp.zeros((ROWS, ROWS), F32)
        for other in range(TOP):
            theirs = column(route_rows[other : other + 1, :], ROWS)
            same = same + jnp.where((theirs == mine) & earlier, 1.0, 0.0)
        targets.append(mine * CAP + jnp.sum(same, axis=0, keepdims=True))
    tall = QCHUNKS * ROWS
    copies = iota((tall, ROWS), 0) % ROWS == iota((tall, ROWS), 1)
    tall_chunk = (iota((tall, 1), 0) // ROWS).astype(F32)
    lane = iota((1, NEP * QMSG), 1)
    lane_key = (((lane // QMSG) * CAP + lane % CAP) * QCHUNKS + (lane % QMSG) // CAP).astype(F32)
    weigh = jnp.zeros((tall, NEP * QMSG), F32)
    filled = jnp.zeros((tall, NEP * QMSG), F32)
    for choice in range(TOP):
        tall_key = (
            jnp.sum(jnp.where(copies, targets[choice], 0.0), axis=1, keepdims=True) * QCHUNKS
            + tall_chunk
        )
        weight = jnp.sum(
            jnp.where(copies, route_weight[choice : choice + 1, :], 0.0), axis=1, keepdims=True
        )
        hit = tall_key == lane_key
        weigh = weigh + jnp.where(hit, weight, 0.0)
        filled = filled + jnp.where(hit, 1.0, 0.0)
    weigh_high = weigh.astype(BF16)
    weigh_low = (weigh - weigh_high.astype(F32)).astype(BF16)
    pick = filled.T.astype(BF16)

    def bytes_of(view, sems):
        return pltpu.make_async_remote_copy(
            src_ref=view,
            dst_ref=view,
            send_sem=sems.at[0],
            recv_sem=sems.at[1],
            device_id=(ep, tp),
            device_id_type=MESH,
        )

    bytes_of(heads.at[pl.ds(0, NTP - 1)], head_sems).wait_recv()
    summed = heads[0].astype(F32)
    for h in range(1, NTP):
        summed = summed + heads[h].astype(F32)
    residual = token_rows + summed
    expert_in = layer_norm(residual, gain_moe[...])
    for q in range(NTP):
        res_buf[q] = residual[:, q * QUARTER : (q + 1) * QUARTER]
        in_buf[q] = expert_in[:, q * QUARTER : (q + 1) * QUARTER]

    def pick_quarter(q):
        stacked = jnp.concatenate(
            [in_buf[q, :, j * LANES : (j + 1) * LANES] for j in range(QCHUNKS)], axis=0
        ).astype(BF16)
        picked = jnp.dot(pick, stacked, preferred_element_type=F32).astype(BF16)
        return picked.reshape(NEP, QMSG, LANES)

    def dispatch(first, last, source, q, sems, far_first):
        def send(k, to):
            pltpu.make_async_remote_copy(
                src_ref=source.at[to],
                dst_ref=rows.at[q, k],
                send_sem=sems.at[0],
                recv_sem=sems.at[1],
                device_id=(to, tp),
                device_id_type=MESH,
            ).start()

        each_partner(ep, 1, first, last, send, far_first)

    disp_send[...] = pick_quarter(tp)
    for group in range(GROUPS):
        dispatch(group * GROUP, (group + 1) * GROUP, disp_send, tp, disp_sems.at[group], False)
    rows[tp, 0] = disp_send[ep]
    disp_opposite[...] = pick_quarter(opposite)
    dispatch(NEP - GROUP // 2, NEP, disp_opposite, opposite, disp_sems.at[GROUPS], True)

    neighbours = (1, NTP - 1)

    def own_bytes(group):
        return bytes_of(
            rows.at[0, pl.ds(0, GROUP - (group == 0))], disp_sems.at[group]
        )

    def spread_bytes(group):
        return bytes_of(rows.at[pl.ds(0, 2), pl.ds(group * GROUP, GROUP)], row_sems.at[group])

    for group in range(GROUPS):
        own_bytes(group).wait_recv()
        block = pl.ds(group * GROUP, GROUP)
        for d in neighbours:
            pltpu.make_async_remote_copy(
                src_ref=rows.at[tp, block],
                dst_ref=rows.at[tp, block],
                send_sem=row_sems.at[group, 0],
                recv_sem=row_sems.at[group, 1],
                device_id=(ep, (tp + d) % NTP),
                device_id_type=MESH,
            ).start()
        if group == 0:
            dispatch(NEP // 2, NEP - GROUP // 2, disp_opposite, opposite, disp_sems.at[GROUPS], True)
        if group == 1:
            dispatch(0, NEP // 2, disp_opposite, opposite, disp_sems.at[GROUPS], True)
            rows[opposite, 0] = disp_opposite[ep]

    for load in loads[6:]:
        load.wait()
    height = NEP * QMSG
    quarters = []

    def absorb(i, q):
        stage[i * height : (i + 1) * height, :] = rows[q].astype(F32).reshape(height, LANES)
        product = jnp.zeros((SLOTS, 2 * HIDDEN), F32)
        for j in range(0, QCHUNKS, 2):
            wide_rows = jnp.concatenate(
                [
                    jnp.concatenate(
                        [
                            stage[
                                pl.ds(
                                    i * height + group * GROUP * QMSG + (j + h) * CAP + c,
                                    GROUP,
                                    stride=QMSG,
                                ),
                                :,
                            ]
                            for group in range(GROUPS)
                            for c in range(CAP)
                        ],
                        axis=0,
                    )
                    for h in range(2)
                ],
                axis=1,
            ).astype(BF16)
            product = product + jnp.dot(
                wide_rows, gu_buf[q, j * LANES : (j + 2) * LANES, :], preferred_element_type=F32
            )
        quarters.append(product)

    opposite_bytes = bytes_of(rows.at[0, pl.ds(0, NEP - 1)], disp_sems.at[GROUPS])
    absorb(0, tp)
    opposite_bytes.wait_recv()
    absorb(1, opposite)
    for group in range(GROUPS):
        spread_bytes(group).wait_recv()
    absorb(2, (tp + 1) % NTP)
    absorb(3, (tp + 3) % NTP)
    gate_up = (quarters[0] + quarters[1]) + (quarters[2] + quarters[3])
    gate_part, up_part = gate_up[:, :HIDDEN], gate_up[:, HIDDEN:]
    hidden = (gate_part / (1.0 + jnp.exp(-gate_part)) * up_part).astype(BF16)

    def partial(q):
        return jnp.dot(hidden, down_buf[q], preferred_element_type=F32)

    def send_part(group, i):
        pltpu.make_async_remote_copy(
            src_ref=part_send.at[group, i],
            dst_ref=part_recv.at[group, i],
            send_sem=part_sems.at[group, 0],
            recv_sem=part_sems.at[group, 1],
            device_id=(ep, (tp + neighbours[i]) % NTP),
            device_id_type=MESH,
        ).start()

    for i in range(2):
        product = partial((tp + neighbours[i]) % NTP).astype(BF16)
        for group in range(GROUPS):
            part_send[group, i] = product[group * GROUP * CAP : (group + 1) * GROUP * CAP]
        send_part(GROUPS - 1, i)
    for group in range(GROUPS - 2, -1, -1):
        for i in range(2):
            send_part(group, i)

    def as_messages(product, group):
        for j in range(QCHUNKS):
            for c in range(CAP):
                ret_stage[pl.ds(group * GROUP * QMSG + j * CAP + c, GROUP, stride=QMSG), :] = (
                    product[c * GROUP : (c + 1) * GROUP, j * LANES : (j + 1) * LANES]
                )
        block = ret_stage[group * GROUP * QMSG : (group + 1) * GROUP * QMSG, :]
        return block.reshape(GROUP, QMSG, LANES).astype(BF16)

    def return_to(source, target, sems, lane_of_tp):
        def send(k, to):
            pltpu.make_async_remote_copy(
                src_ref=source.at[k],
                dst_ref=target.at[ep],
                send_sem=sems.at[0],
                recv_sem=sems.at[1],
                device_id=(to, lane_of_tp),
                device_id_type=MESH,
            ).start()

        return send

    product = partial(opposite)
    for group in range(GROUPS):
        opp_send[group * GROUP : (group + 1) * GROUP] = as_messages(
            product[group * GROUP * CAP : (group + 1) * GROUP * CAP], group
        )
    each_partner(ep, -1, 0, NEP, return_to(opp_send, opp_recv, ret_sems.at[1], tp), True)
    opp_recv[ep] = opp_send[0]

    own = partial(tp)
    send_own = return_to(ret_send, ret_recv, ret_sems.at[0], tp)
    for group in range(GROUPS - 1, -1, -1):
        bytes_of(part_recv.at[group], part_sems.at[group]).wait_recv()
        total = own[group * GROUP * CAP : (group + 1) * GROUP * CAP]
        for i in range(2):
            total = total + part_recv[group, i].astype(F32)
        ret_send[group * GROUP : (group + 1) * GROUP] = as_messages(total, group)
        each_partner(ep, -1, group * GROUP, (group + 1) * GROUP, send_own, True)
    ret_recv[ep] = ret_send[0]


    def weighted(buffer):
        returned = buffer[...].astype(F32).reshape(NEP * QMSG, LANES).astype(BF16)
        return jnp.dot(weigh_high, returned, preferred_element_type=F32) + jnp.dot(
            weigh_low, returned, preferred_element_type=F32
        )

    back = [
        bytes_of(buffer.at[pl.ds(0, NEP - 1)], ret_sems.at[i])
        for i, buffer in enumerate((ret_recv, opp_recv))
    ]
    back[1].wait_recv()
    cross_send[...] = weighted(opp_recv)
    cross = pltpu.make_async_remote_copy(
        src_ref=cross_send,
        dst_ref=cross_recv,
        send_sem=ret_sems.at[2, 0],
        recv_sem=ret_sems.at[2, 1],
        device_id=(ep, opposite),
        device_id_type=MESH,
    )
    cross.start()
    bytes_of(heads.at[pl.ds(0, NTP - 1)], head_sems).wait_send()
    for group in range(GROUPS):
        own_bytes(group).wait_send()
        spread_bytes(group).wait_send()
        bytes_of(part_recv.at[group], part_sems.at[group]).wait_send()
    opposite_bytes.wait_send()
    back[0].wait_recv()
    combined = weighted(ret_recv)
    cross.wait_recv()
    combined = combined + cross_recv[...]
    for j in range(QCHUNKS):
        output[:, j * LANES : (j + 1) * LANES] = (
            res_buf[tp, :, j * LANES : (j + 1) * LANES] + combined[j * ROWS : (j + 1) * ROWS]
        ).astype(BF16)
    stores[0].start()
    cross.wait_send()
    for messages in back:
        messages.wait_send()
    for store in stores:
        store.wait()


def update_kernel(
    admitted_in,
    values_in,
    keep_in,
    memory,
    output_in,
    norm_in,
    stab_in,
    memory_next,
    output,
    norm_next,
    stabilizer_next,
    admitted,
    values,
    keep,
    mem_buf,
    output_buf,
    norm_buf,
    stab_buf,
    load_sem,
    store_sem,
):
    loads = [
        pltpu.make_async_copy(source, target, load_sem.at[i])
        for i, (source, target) in enumerate(
            (
                (admitted_in, admitted),
                (values_in, values),
                (keep_in, keep),
                (output_in, output_buf),
                (norm_in, norm_buf),
                (stab_in, stab_buf),
            )
        )
    ]
    blocks = [
        pltpu.make_async_copy(memory.at[s, 0], mem_buf.at[s], load_sem.at[6 + s])
        for s in range(ROWS)
    ]
    for load in loads + blocks:
        load.start()
    passed = [
        pltpu.make_async_copy(source, target, store_sem.at[ROWS + i])
        for i, (source, target) in enumerate(
            ((output_buf, output), (norm_buf, norm_next), (stab_buf, stabilizer_next))
        )
    ]
    for load in loads[:3]:
        load.wait()
    admitted_t = admitted[...].T
    for load, store in zip(loads[3:], passed, strict=True):
        load.wait()
        store.start()
    stores = []
    for s in range(ROWS):
        blocks[s].wait()
        mem_buf[s] = (
            keep[s : s + 1, 0:1] * mem_buf[s] + admitted_t[:, s : s + 1] * values[s : s + 1, :]
        )
        store = pltpu.make_async_copy(mem_buf.at[s], memory_next.at[s, 0], store_sem.at[s])
        store.start()
        stores.append(store)
    for store in passed + stores:
        store.wait()


def shards(
    tokens,
    w_query,
    w_key,
    w_value,
    w_outgate,
    w_igate,
    w_fgate,
    forget_bias,
    w_out,
    gain_mix,
    gain_moe,
    memory,
    normalizer,
    stabilizer,
    expert_gate,
    expert_up,
    expert_down,
    routes,
    route_weight,
):
    vmem = pl.BlockSpec(memory_space=pltpu.VMEM)
    smem = pl.BlockSpec(memory_space=pltpu.SMEM)
    hbm = pl.BlockSpec(memory_space=pl.ANY)
    smalls = (
        tokens,
        gain_mix.reshape(1, WIDTH),
        gain_moe.reshape(1, WIDTH),
        w_igate.reshape(1, WIDTH),
        w_fgate.reshape(1, WIDTH),
        normalizer,
        stabilizer.reshape(1, ROWS),
        routes.T,
        route_weight.T,
    )
    norm_shape = jax.ShapeDtypeStruct(normalizer.shape, F32)
    output_shape = jax.ShapeDtypeStruct((ROWS, QUARTER), BF16)
    stab_shape = jax.ShapeDtypeStruct((1, ROWS), F32)
    row_shape = jax.ShapeDtypeStruct((ROWS, HEAD), F32)
    keep_shape = jax.ShapeDtypeStruct((ROWS, LANES), F32)
    message = (QMSG, LANES)
    results = (output_shape, row_shape, row_shape, keep_shape, norm_shape, stab_shape)
    output, admitted, values, keep, norm_next, stab = pl.pallas_call(
        kernel,
        out_shape=results,
        in_specs=[hbm] * 18 + [smem],
        out_specs=(hbm,) * 6,
        scratch_shapes=[pltpu.VMEM(x.shape, x.dtype) for x in (*results, *smalls)]
        + [
            pltpu.VMEM((4, WIDTH, HEAD), BF16),
            pltpu.VMEM((ROWS, HEAD, HEAD), F32),
            pltpu.VMEM((HEAD, WIDTH), BF16),
            pltpu.VMEM((NTP, QUARTER, 2 * HIDDEN), BF16),
            pltpu.VMEM((NTP, HIDDEN, QUARTER), BF16),
            pltpu.VMEM((ROWS, HEAD), F32),
            pltpu.VMEM((NTP, ROWS, QUARTER), F32),
            pltpu.VMEM((NTP, ROWS, QUARTER), F32),
            pltpu.VMEM((NTP, ROWS, WIDTH), BF16),
            pltpu.VMEM((NTP * NEP * QMSG, LANES), F32),
            pltpu.VMEM((NEP, *message), BF16),
            pltpu.VMEM((NEP, *message), BF16),
            pltpu.VMEM((NTP, NEP, *message), BF16),
            pltpu.VMEM((GROUPS, 2, GROUP * CAP, QUARTER), BF16),
            pltpu.VMEM((GROUPS, 2, GROUP * CAP, QUARTER), BF16),
            pltpu.VMEM((NEP * QMSG, LANES), F32),
            pltpu.VMEM((NEP, *message), BF16),
            pltpu.VMEM((NEP, *message), BF16),
            pltpu.VMEM((NEP, *message), BF16),
            pltpu.VMEM((NEP, *message), BF16),
            pltpu.VMEM((QCHUNKS * ROWS, LANES), F32),
            pltpu.VMEM((QCHUNKS * ROWS, LANES), F32),
            pltpu.SemaphoreType.DMA((9,)),
            pltpu.SemaphoreType.DMA((12,)),
            pltpu.SemaphoreType.DMA((2,)),
            pltpu.SemaphoreType.DMA((GROUPS + 1, 2)),
            pltpu.SemaphoreType.DMA((GROUPS, 2)),
            pltpu.SemaphoreType.DMA((GROUPS, 2)),
            pltpu.SemaphoreType.DMA((3, 2)),
            pltpu.SemaphoreType.DMA((6,)),
        ],
        compiler_params=pltpu.CompilerParams(
            collective_id=0, has_side_effects=True, vmem_limit_bytes=60 * 1024 * 1024
        ),
        name="layer",
    )(
        *smalls,
        w_key,
        w_value,
        w_query,
        w_outgate,
        memory,
        w_out,
        expert_gate.reshape(NTP, QUARTER, HIDDEN),
        expert_up.reshape(NTP, QUARTER, HIDDEN),
        expert_down,
        forget_bias,
    )
    memory_next, output, norm_next, stab = pl.pallas_call(
        update_kernel,
        out_shape=(
            jax.ShapeDtypeStruct(memory.shape, F32),
            output_shape,
            norm_shape,
            stab_shape,
        ),
        in_specs=[hbm] * 7,
        out_specs=(hbm,) * 4,
        scratch_shapes=[
            pltpu.VMEM((ROWS, HEAD), F32),
            pltpu.VMEM((ROWS, HEAD), F32),
            pltpu.VMEM((ROWS, LANES), F32),
            pltpu.VMEM((ROWS, HEAD, HEAD), F32),
            pltpu.VMEM(output_shape.shape, BF16),
            pltpu.VMEM(norm_shape.shape, F32),
            pltpu.VMEM(stab_shape.shape, F32),
            pltpu.SemaphoreType.DMA((6 + ROWS,)),
            pltpu.SemaphoreType.DMA((ROWS + 3,)),
        ],
        compiler_params=pltpu.CompilerParams(vmem_limit_bytes=60 * 1024 * 1024),
        name="update",
    )(admitted, values, keep, memory, output, norm_next, stab)
    return output, memory_next, norm_next, stab.reshape(ROWS, 1)


def solution(mesh):
    return jax.shard_map(
        shards,
        mesh=mesh,
        in_specs=(
            P("ep", None),
            P(None, "tp"),
            P(None, "tp"),
            P(None, "tp"),
            P(None, "tp"),
            P(None, "tp"),
            P(None, "tp"),
            P("tp"),
            P("tp", None),
            P(),
            P(),
            P("ep", "tp", None, None),
            P("ep", "tp", None),
            P("ep", "tp"),
            P("ep", None, "tp"),
            P("ep", None, "tp"),
            P("ep", "tp", None),
            P("ep", None),
            P("ep", None),
        ),
        out_specs=(P("ep", "tp"), P("ep", "tp", None, None), P("ep", "tp", None), P("ep", "tp")),
        check_vma=False,
    )
```
